256 devices in a mesh: sp: 64 (over z, x, core), tp: 4 (over y).
Axes of the slice: x: 4, y: 4, z: 8, core: 2. Of those that a mesh axis runs over, the one named last changes fastest.
Arguments:
- cot_out: bfloat16 [16384, 2048], P('sp', 'tp'), may hold values from -16 to 16
- route_ids: int32 [16384, 2], P('sp'), may hold values from 0 to 63, all different within a row; in each aligned block of 256 rows (0 to 255, 256 to 511, ...) at most 12 rows name the same one
- route_weight: float32 [16384, 2], P('sp'), may hold values from 0.1 to 1
- expert_inputs: bfloat16 [64, 768, 2048], P('sp'), may hold values from -48 to 48
- w_gate: bfloat16 [64, 2048, 1024], P('sp', None, 'tp'), may hold values from -0.125 to 0.125
- w_up: bfloat16 [64, 2048, 1024], P('sp', None, 'tp'), may hold values from -0.125 to 0.125
- w_down: bfloat16 [64, 1024, 2048], P('sp', 'tp'), may hold values from -0.1875 to 0.1875
- w_proj: bfloat16 [2048, 2048], P('tp'), may hold values from -0.125 to 0.125
- conv_out: bfloat16 [16384, 2048], P('sp', 'tp'), may hold values from -6 to 6
- channel_norm_gain: float32 [2048], P('tp'), may hold values from 0.1 to 1.9
- taps: float32 [31, 2048], P(None, 'tp'), may hold values from -1 to 1
- value_pre: bfloat16 [16384, 2048], P('sp', 'tp'), may hold values from -6 to 6
- gate_pre: bfloat16 [16384, 2048], P('sp', 'tp'), may hold values from -6 to 6
Outputs:
- grad_gate_w: bfloat16 [64, 2048, 1024], P('sp', None, 'tp')
- grad_up_w: bfloat16 [64, 2048, 1024], P('sp', None, 'tp')
- grad_down_w: bfloat16 [64, 1024, 2048], P('sp', 'tp')
- grad_proj: float32 [2048, 2048], P(('tp', 'sp'))
- grad_value: bfloat16 [16384, 2048], P('sp', 'tp')
- grad_gate: bfloat16 [16384, 2048], P('sp', 'tp')
The draws below stay inside these ranges and needn't reach their ends.
Inputs may be any that keep to these rules, and one draw needn't show every extreme that they name: `route_ids`: among the tokens of one index of sp no expert is chosen more than 12 times, a bound that some block reaches; a token's experts differ.
All inputs are finite; a program needn't handle non-finite values.
Results may differ from the reference program's by a relative error of at most 0.012.
Values may be sent and summed in bfloat16 or wider, within the bound.
A program may use at most 128 MiB of HBM per device.

```python
import math
import jax
import jax.numpy as jnp
import numpy as np
from jax import lax

D = 2048
F = 1024
WIDTH = 31
TOP = 2
TOK_DEV = 256
EXPERTS = 64
CAP = 12
SLOTS = 768
TOKENS = 16384
N_SP = 64
N_TP = 4


def draw_expert_inputs(key, part):
    keys = jax.random.split(jax.random.fold_in(key, 11), 2)
    shape = (EXPERTS, SLOTS, D)
    base = jax.random.truncated_normal(keys[0], -6.0, 6.0, shape, jnp.float32)
    scales = jnp.exp(jax.random.uniform(keys[1], (EXPERTS, SLOTS, 1), jnp.float32, jnp.log(0.5), jnp.log(6.0)))
    values = scales * base
    return jnp.clip(values, -48.0, 48.0).astype(jnp.bfloat16)


def spiked(values, own_key, source, target, parts, factor):
    def block_of(position):
        return (jnp.arange(values.shape[position]) // (values.shape[position] // parts)).reshape((-1,) + (1,) * (values.ndim - 1 - position))

    near = jax.random.permutation(own_key, parts)[block_of(target)]
    second = (block_of(target) + parts // 2) % parts
    return jnp.where((block_of(source) == near) | (block_of(source) == second), factor * values, values)


def level_of(own_key, dims, pieces, least, top_value):
    def one(axis_at, blocks):
        draws = jax.random.uniform(jax.random.fold_in(jax.random.fold_in(own_key, 6), axis_at), (blocks,), jnp.float32, least / len(pieces), top_value / len(pieces))
        return jnp.repeat(jnp.exp(draws), dims[axis_at] // blocks).reshape((-1,) + (1,) * (len(dims) - axis_at - 1))

    gain = one(*pieces[0])
    for cut in pieces[1:]:
        gain = gain * one(*cut)
    return gain


def shared_out(stream_key, own, number, rows, count, top, reach, lean):
    ranking = jax.random.permutation(stream_key, count)
    heavy_load, usual = shares(count, rows * top, reach, lean, True), shares(count, rows * top, reach, lean, False)
    places = jnp.arange(count)

    def named(tallies, offset_by):
        used = int((tallies > 0).sum())
        fixed = max(1, used // 4)
        passed = fixed + (places - fixed + offset_by * (used - fixed)) % max(1, count - fixed)
        return jnp.zeros((count,), jnp.int32).at[ranking[jnp.where(places < fixed, places, passed)]].set(jnp.asarray(tallies, jnp.int32))

    tallies = jnp.where(number % 4 == 0, named(heavy_load, number // 4), named(usual, number - number // 4 - 1))
    mixed = jax.random.permutation(jax.random.fold_in(own, 3), count)
    source_of, sink = mixed[0:count // 2 * 2:2], mixed[1:count // 2 * 2:2]
    room = jnp.minimum(tallies[source_of] - 1, reach - tallies[sink]) // 2
    room = jnp.where((source_of == ranking[0]) | (sink == ranking[0]) | (tallies[sink] == 0), 0, jnp.maximum(room, 0))
    passed = jax.random.randint(jax.random.fold_in(own, 4), (count // 2,), 0, 1 << 20) % (room + 1)
    tallies = tallies.at[source_of].add(-passed).at[sink].add(passed)
    members = jnp.searchsorted(jnp.cumsum(tallies), jnp.arange(rows * top), side="right").astype(jnp.int32)
    table = members.reshape(top, rows).T
    table = table[jax.random.permutation(jax.random.fold_in(own, 1), rows)]
    offset_by = jax.random.randint(jax.random.fold_in(own, 2), (rows, 1), 0, top)
    return jnp.take_along_axis(table, (jnp.arange(top)[None, :] + offset_by) % top, axis=1)


def shares(amount, total, limit, lean, full):
    portions = [(1 << 20) // math.isqrt(grade ** lean) + 1 for grade in range(1, amount + 1)]
    largest = limit if full else min(limit, max(-(-total // amount), total * portions[0] // sum(portions)))
    least = 1 if total - largest >= amount - 1 else 0
    given, rest = [largest] + [least] * (amount - 1), total - largest - least * (amount - 1)
    while rest > 0:
        free = [i for i in range(1, amount) if given[i] < largest] or [i for i in range(1, amount) if given[i] < limit]
        whole, budget = sum([portions[i] for i in free]), rest
        for i in free:
            extra = min(limit - given[i], max(1, budget * portions[i] // whole), rest)
            given[i] = given[i] + extra
            rest = rest - extra
    return np.array(given)


def centred(key, dims, width, most, cuts=(), held_as=jnp.bfloat16):
    drawn = jax.random.normal(key, dims, jnp.float32) * width
    if len(cuts) > 0:
        drawn = level_of(key, dims, cuts, -0.22, 0.18) * drawn
    return jnp.clip(drawn, min=-most, max=most).astype(held_as)


def gaussian_with(key, shape, spread, reach, shards, heavy, held_as=jnp.bfloat16):
    drawn = spread * jax.random.normal(key, shape, jnp.float32)
    if shards:
        drawn = drawn * level_of(key, shape, shards, -0.22, 0.18)
    return jnp.clip(spiked(drawn, jax.random.fold_in(key, 3), *heavy), -reach, reach).astype(held_as)


def setup_inputs(seed: int = 0) -> dict:
    seeds = jax.random.split(jax.random.key(seed), 14)
    cot_out = gaussian_with(seeds[0], (TOKENS, D), 1.0, 16.0, ((0, 64), (1, 4)), (0, 1, 64, 4.0))
    route_ids_keys = jax.random.split(jax.random.fold_in(seeds[1], 1), TOKENS // TOK_DEV)
    route_ids_turns = jax.random.permutation(jax.random.fold_in(seeds[1], 3), TOKENS // TOK_DEV)
    route_ids = jax.vmap(lambda own, number: shared_out(jax.random.fold_in(seeds[1], 2), own, number, TOK_DEV, EXPERTS, TOP, CAP, 2))(route_ids_keys, route_ids_turns).reshape((TOKENS, TOP))
    route_weight = jnp.clip(jnp.exp(math.log(1.0) - 2.3025851 * jax.random.uniform(seeds[2], (TOKENS, TOP), jnp.float32) ** level_of(seeds[2], (TOKENS, TOP), ((0, 64),), -0.2, 0.2)), 0.1, 1.0)
    expert_inputs = draw_expert_inputs(jax.random.fold_in(seeds[13], 71), 0)
    w_gate = centred(seeds[4], (EXPERTS, D, F), D ** -0.5, 0.125, ((0, 64), (2, 4)))
    w_up = centred(seeds[5], (EXPERTS, D, F), D ** -0.5, 0.125, ((0, 64), (2, 4)))
    w_down = centred(seeds[6], (EXPERTS, F, D), F ** -0.5, 0.1875, ((0, 64), (1, 4)))
    w_proj = centred(seeds[7], (D, D), D ** -0.5, 0.125, ((0, 4),))
    conv_out = centred(seeds[8], (TOKENS, D), 1.0, 6.0, ((0, 64), (1, 4)))
    channel_norm_gain = jnp.clip(1.0 + 0.18 * jax.random.normal(seeds[9], (D,), jnp.float32), 0.1, 1.9)
    taps = centred(seeds[10], (WIDTH, D), WIDTH ** -0.5, 1.0, ((1, 4),), jnp.float32)
    value_pre = centred(seeds[11], (TOKENS, D), 1.0, 6.0, ((0, 64), (1, 4)))
    gate_pre = centred(seeds[12], (TOKENS, D), 1.5, 6.0, ((0, 64), (1, 4)))
    return dict(cot_out=cot_out, route_ids=route_ids, route_weight=route_weight, expert_inputs=expert_inputs, w_gate=w_gate, w_up=w_up, w_down=w_down, w_proj=w_proj, conv_out=conv_out, channel_norm_gain=channel_norm_gain, taps=taps, value_pre=value_pre, gate_pre=gate_pre)


clamp_limit = 7.0
swish_alpha = 1.702
norm_epsilon = 1e-05

def one_expert(operands):
    rows_in, rows_cot, gate_weight, up_weight, down_weight = operands
    gate_lin = jnp.dot(rows_in, gate_weight, preferred_element_type=jnp.float32)
    up_lin = jnp.dot(rows_in, up_weight, preferred_element_type=jnp.float32)
    gate_c = jnp.minimum(gate_lin, clamp_limit)
    up_c = jnp.clip(up_lin, -clamp_limit, clamp_limit)
    sig = jax.nn.sigmoid(swish_alpha * gate_c)
    act = ((up_c + 1.0) * gate_c * sig).astype(jnp.bfloat16)
    grad_down = jnp.dot(act.T, rows_cot, preferred_element_type=jnp.float32).astype(jnp.bfloat16)
    d_act = jnp.dot(rows_cot, down_weight.T, preferred_element_type=jnp.float32)
    up_open = ((up_lin > -clamp_limit) & (up_lin < clamp_limit)).astype(jnp.float32)
    gate_open = (gate_lin < clamp_limit).astype(jnp.float32)
    d_up = (d_act * gate_c * sig * up_open).astype(jnp.bfloat16)
    d_gate = (d_act * (up_c + 1.0) * (sig + swish_alpha * gate_c * sig * (1.0 - sig)) * gate_open).astype(jnp.bfloat16)
    grad_gate = jnp.dot(rows_in.T, d_gate, preferred_element_type=jnp.float32).astype(jnp.bfloat16)
    grad_up = jnp.dot(rows_in.T, d_up, preferred_element_type=jnp.float32).astype(jnp.bfloat16)
    blocks = F // N_TP
    gate_parts = jnp.einsum('snf,dnf->nsd', d_gate.reshape(SLOTS, N_TP, blocks).astype(jnp.float32), gate_weight.reshape(D, N_TP, blocks).astype(jnp.float32))
    up_parts = jnp.einsum('snf,dnf->nsd', d_up.reshape(SLOTS, N_TP, blocks).astype(jnp.float32), up_weight.reshape(D, N_TP, blocks).astype(jnp.float32))
    rounded = (gate_parts + up_parts).astype(jnp.bfloat16)
    rounded = lax.optimization_barrier(rounded)
    input_grad = lax.optimization_barrier(jnp.sum(rounded.astype(jnp.float32), axis=0)).astype(jnp.bfloat16)
    return (grad_gate, grad_up, grad_down, input_grad)

def reference(cot_out, route_ids, route_weight, expert_inputs, w_gate, w_up, w_down, w_proj, conv_out, channel_norm_gain, taps, value_pre, gate_pre):
    block_ids = route_ids.reshape(N_SP, TOK_DEV * TOP)
    expert_hot = (block_ids[:, :, None] == jnp.arange(EXPERTS, dtype=jnp.int32)[None, None, :]).astype(jnp.int32)
    earlier = lax.optimization_barrier(jnp.sum((jnp.cumsum(expert_hot, axis=1) - expert_hot) * expert_hot, axis=2))
    dest_slot = (jnp.arange(N_SP, dtype=jnp.int32)[:, None] * CAP + earlier).reshape(-1).astype(jnp.int32)
    expert_of = block_ids.reshape(-1).astype(jnp.int32)
    repeated = jnp.repeat(cot_out, TOP, axis=0).astype(jnp.float32)
    scaled = (route_weight.reshape(-1)[:, None] * repeated).astype(jnp.bfloat16)
    expert_cot = jnp.zeros((EXPERTS, SLOTS, D), jnp.bfloat16).at[expert_of, dest_slot].set(scaled)
    grad_gate_w, grad_up_w, grad_down_w, expert_grad = lax.map(one_expert, (expert_inputs, expert_cot, w_gate, w_up, w_down))
    picked = expert_grad[expert_of, dest_slot].astype(jnp.float32).reshape(TOKENS, TOP, D)
    mix_grad = (cot_out.astype(jnp.float32) + lax.optimization_barrier(jnp.sum(picked, axis=1))).astype(jnp.bfloat16)
    convolution_filter = conv_out.astype(jnp.float32)
    channel_mean = lax.optimization_barrier(jnp.mean(convolution_filter, axis=1, keepdims=True))
    var = lax.optimization_barrier(jnp.mean(convolution_filter * convolution_filter, axis=1, keepdims=True)) - channel_mean * channel_mean
    inverse_deviation = lax.rsqrt(var + norm_epsilon)
    normalized_input = (convolution_filter - channel_mean) * inverse_deviation
    normalized_output = normalized_input * channel_norm_gain[None, :]
    sig = jax.nn.sigmoid(normalized_output)
    act_conv = (normalized_output * sig).astype(jnp.bfloat16)
    grad_proj = jnp.dot(act_conv.T, mix_grad, preferred_element_type=jnp.float32)
    d_act_conv = jnp.dot(mix_grad, w_proj.T, preferred_element_type=jnp.float32)
    normalized_gradient = d_act_conv * sig * (1.0 + normalized_output * (1.0 - sig)) * channel_norm_gain[None, :]
    first_moment_mean = lax.optimization_barrier(jnp.mean(normalized_gradient, axis=1, keepdims=True))
    second_moment_mean = lax.optimization_barrier(jnp.mean(normalized_gradient * normalized_input, axis=1, keepdims=True))
    convolution_gradient = inverse_deviation * (normalized_gradient - first_moment_mean - normalized_input * second_moment_mean)
    extended = jnp.concatenate([convolution_gradient, jnp.zeros((WIDTH - 1, D), jnp.float32)], axis=0)
    d_glu = jnp.zeros((TOKENS, D), jnp.float32)
    for offset in range(WIDTH):
        begin = WIDTH - 1 - offset
        d_glu = d_glu + taps[offset][None, :] * extended[begin:begin + TOKENS]
    gate_sig = jax.nn.sigmoid(gate_pre.astype(jnp.float32))
    grad_value = (d_glu * gate_sig).astype(jnp.bfloat16)
    grad_gate = (d_glu * value_pre.astype(jnp.float32) * gate_sig * (1.0 - gate_sig)).astype(jnp.bfloat16)
    return (grad_gate_w, grad_up_w, grad_down_w, grad_proj, grad_value, grad_gate)
```

```python
import jax
import jax.numpy as jnp
from jax import lax
from jax.experimental import pallas as pl
from jax.experimental.pallas import tpu as pltpu
from jax.sharding import Mesh
from jax.sharding import PartitionSpec as P

SP = ("sp_0", "sp_1", "sp_2")
TP_SP = ("tp", "sp_0", "sp_1", "sp_2")
MESH = pl.DeviceIdType.MESH

clamp_limit = 7.0
swish_alpha = 1.702
norm_epsilon = 1e-05

CH = 4
LANES = 128
NZ = 8
NG = 8
NY = 4
CAP = 12
BLOCK = NZ * CAP
ROWS = NZ * BLOCK
HALF = ROWS // 2
TOK = 256
WIDE = CH * LANES
HID = 256
BF = jnp.bfloat16
F32 = jnp.float32


def nt(a, b):
    return lax.dot_general(a, b, (((1,), (1,)), ((), ())), preferred_element_type=F32)


def tn(a, b):
    return lax.dot_general(a, b, (((0,), (0,)), ((), ())), preferred_element_type=F32)


def nn(a, b):
    return lax.dot_general(a, b, (((1,), (0,)), ((), ())), preferred_element_type=F32)


def wait_all(ref, sem):
    pltpu.make_async_copy(ref, ref, sem).wait()


def send(src, dst, send_sem, recv_sem, device):
    pltpu.make_async_remote_copy(
        src_ref=src,
        dst_ref=dst,
        send_sem=send_sem,
        recv_sem=recv_sem,
        device_id=device,
        device_id_type=MESH,
    ).start()


def lanes(c):
    return pl.ds(c * LANES, LANES)


def rows_of(block):
    return pl.ds(pl.multiple_of(block * BLOCK, BLOCK), BLOCK)


def moe_kernel(
    cot, ids_c, ids_r, w_r, rows_in, wg, wu, wd, perm,
    gg_out, gu_out, gd_out, mix,
    out_a, recv_a, out_b, cotf, act_s, f_up, f_gate, dact, dgu, sel_t, rows_p,
    partial, r1l, r1r, accl, accr, from_l, from_r, egrad, recv_b2, out_a2, coming,
    s_a, r_a, s_b, r_b, s_y, r_yl, r_yr, r_fl, r_fr,
    s_rs, r_1l, r_1r, r_sl, r_sr, s_b2, r_b2, s_a2, r_a2, s_m, r_ml, r_mr, r_nl, r_nr,
):
    z = lax.axis_index("sp_0")
    g = lax.axis_index("sp_1") * 2 + lax.axis_index("sp_2")
    y = lax.axis_index("tp")
    right, left, across = lax.rem(y + 1, NY), lax.rem(y + 3, NY), lax.rem(y + 2, NY)
    to_right, to_left = {"tp": right}, {"tp": left}

    def z_peer(step):
        peer = lax.rem(z + step, NZ)
        return peer, {"sp_0": peer}

    def g_peer(step):
        peer = lax.rem(g + step, NG)
        return peer, {"sp_1": peer // 2, "sp_2": lax.rem(peer, 2)}

    barrier = pltpu.get_barrier_semaphore()
    for step in range(1, NZ):
        pl.semaphore_signal(barrier, inc=1, device_id=z_peer(step)[1], device_id_type=MESH)
        pl.semaphore_signal(barrier, inc=1, device_id=g_peer(step)[1], device_id_type=MESH)
    for device in (to_right, to_left):
        pl.semaphore_signal(barrier, inc=1, device_id=device, device_id_type=MESH)

    t_sub = lax.broadcasted_iota(jnp.int32, (TOK, TOK), 0)
    t_lane = lax.broadcasted_iota(jnp.int32, (TOK, TOK), 1)
    before, after = t_sub < t_lane, t_lane < t_sub
    col = [ids_c[:, k : k + 1] for k in (0, 1)]
    row = [ids_r[k : k + 1, :] for k in (0, 1)]
    slot_r = lax.broadcasted_iota(jnp.int32, (ROWS, TOK), 0).astype(F32)
    slot_c = lax.broadcasted_iota(jnp.int32, (TOK, ROWS), 1).astype(F32)
    chosen, weight, back = None, None, None
    for k in (0, 1):
        same = ((col[0] == row[k]) | (col[1] == row[k])) & before
        dest = jnp.sum(jnp.where(same, 1.0, 0.0), axis=0, keepdims=True) + CAP * row[k]
        hot = slot_r == dest
        one, scale = jnp.where(hot, 1.0, 0.0), jnp.where(hot, w_r[k : k + 1, :], 0.0)
        chosen = one if chosen is None else chosen + one
        weight = scale if weight is None else weight + scale
        same = ((row[0] == col[k]) | (row[1] == col[k])) & after
        dest = jnp.sum(jnp.where(same, 1.0, 0.0), axis=1, keepdims=True) + CAP * col[k]
        one = jnp.where(slot_c == dest, 1.0, 0.0)
        back = one if back is None else back + one
    chosen = chosen.astype(BF)
    weight = jnp.sum(weight, axis=1, keepdims=True)
    sel_t[...] = back.astype(BF)

    pl.semaphore_wait(barrier, NZ - 1 + NG - 1 + 2)

    for c in range(CH):
        picked = nn(chosen, cot[:, lanes(c)])
        out_a[c] = (weight * picked).astype(BF)
        for step in (4, 3, 5, 2, 6, 1, 7):
            peer, device = z_peer(step)
            send(out_a.at[c, rows_of(peer)], recv_a.at[c, rows_of(z)], s_a.at[c], r_a.at[c], device)
        recv_a[c, rows_of(z), :] = out_a[c, rows_of(z), :]

    for j in range(8):
        cols = pl.ds(j * 256, 256)
        rows_p[:, cols] = nn(perm[...], rows_in[:, cols]).astype(BF)
    for j in range(3):
        part = pl.ds(j * 256, 256)
        gate_lin = nn(rows_p[part, :], wg[...])
        up_lin = nn(rows_p[part, :], wu[...])
        gate_c = jnp.minimum(gate_lin, clamp_limit)
        up_c = jnp.clip(up_lin, -clamp_limit, clamp_limit)
        sig = jax.nn.sigmoid(swish_alpha * gate_c)
        act_s[part, :] = ((up_c + 1.0) * gate_c * sig).astype(BF)
        up_open = (up_lin > -clamp_limit) & (up_lin < clamp_limit)
        f_up[part, :] = jnp.where(up_open, gate_c * sig, 0.0)
        slope = (up_c + 1.0) * (sig + swish_alpha * gate_c * sig * (1.0 - sig))
        f_gate[part, :] = jnp.where(gate_lin < clamp_limit, slope, 0.0)

    for s in range(CH + 3):
        c = s
        if 0 <= c < CH:
            wait_all(recv_a.at[c, pl.ds(0, ROWS - BLOCK)], r_a.at[c])
            out_b[c] = nn(perm[...], recv_a[c]).astype(BF)
            for step in (4, 2, 6, 3, 5, 1, 7):
                peer, device = g_peer(step)
                send(
                    out_b.at[c, rows_of(peer)], cotf.at[y, rows_of(g), lanes(c)],
                    s_b.at[c], r_b.at[c], device,
                )
            cotf[y, rows_of(g), lanes(c)] = out_b[c, rows_of(g), :]
        c = s - 1
        if 0 <= c < CH:
            wait_all(out_b.at[c, pl.ds(0, ROWS - BLOCK)], r_b.at[c])
            mine = cotf.at[y, :, lanes(c)]
            send(mine, mine, s_y.at[0, c], r_yl.at[c], to_right)
            send(mine, mine, s_y.at[1, c], r_yr.at[c], to_left)
        c = s - 2
        if 0 <= c < CH:
            wait_all(out_b.at[c], r_yl.at[c])
            passed = cotf.at[left, pl.ds(0, HALF), lanes(c)]
            send(passed, passed, s_y.at[2, c], r_fl.at[c], to_right)
            wait_all(out_b.at[c], r_yr.at[c])
            passed = cotf.at[right, pl.ds(HALF, HALF), lanes(c)]
            send(passed, passed, s_y.at[3, c], r_fr.at[c], to_left)
        c = s - 3
        if 0 <= c < CH:
            wait_all(out_b.at[c, pl.ds(0, HALF)], r_fl.at[c])
            wait_all(out_b.at[c, pl.ds(0, HALF)], r_fr.at[c])
            arrived = jnp.concatenate([cotf[q, :, lanes(c)] for q in range(NY)], axis=1)
            down = jnp.concatenate(
                [wd[:, pl.ds(q * WIDE + c * LANES, LANES)] for q in range(NY)], axis=1
            )
            term = nt(arrived, down)
            dact[...] = term if c == 0 else dact[...] + term

    dgu[:, 0:HID] = (dact[...] * f_gate[...]).astype(BF)
    dgu[:, HID : 2 * HID] = (dact[...] * f_up[...]).astype(BF)

    for c in range(CH):
        weights = jnp.concatenate(
            [
                jnp.concatenate([w[pl.ds(q * WIDE + c * LANES, LANES), :] for w in (wg, wu)], axis=1)
                for q in range(NY)
            ],
            axis=0,
        )
        product = nt(dgu[...], weights).astype(BF)
        for q in range(NY):
            partial[c, q] = product[:, q * LANES : (q + 1) * LANES]
        low, high = pl.ds(0, HALF), pl.ds(HALF, HALF)
        send(partial.at[c, across, low], r1l.at[c], s_rs.at[0, c], r_1l.at[c], to_right)
        send(partial.at[c, across, high], r1r.at[c], s_rs.at[1, c], r_1r.at[c], to_left)
        send(partial.at[c, right, high], from_l.at[c, high], s_rs.at[2, c], r_sl.at[c], to_right)
        send(partial.at[c, left, low], from_r.at[c, low], s_rs.at[3, c], r_sr.at[c], to_left)

    def weight_grads(j):
        if j < 4:
            gd_out[:, pl.ds(j * WIDE, WIDE)] = tn(act_s[...], cotf[j]).astype(BF)
        else:
            part = pl.ds((j - 4) * 256, 256)
            both = tn(rows_p[:, part], dgu[...]).astype(BF)
            gg_out[part, :] = both[:, 0:HID]
            gu_out[part, :] = both[:, HID : 2 * HID]

    work = 0
    for s in range(CH + 5):
        c = s
        if 0 <= c < CH:
            low, high = pl.ds(0, HALF), pl.ds(HALF, HALF)
            wait_all(r1l.at[c], r_1l.at[c])
            accr[c] = (partial[c, right, low, :].astype(F32) + r1l[c].astype(F32)).astype(BF)
            send(accr.at[c], from_l.at[c, low], s_rs.at[4, c], r_sl.at[c], to_right)
            wait_all(r1r.at[c], r_1r.at[c])
            accl[c] = (partial[c, left, high, :].astype(F32) + r1r[c].astype(F32)).astype(BF)
            send(accl.at[c], from_r.at[c, high], s_rs.at[5, c], r_sr.at[c], to_left)
        c = s - 1
        if 0 <= c < CH:
            wait_all(from_l.at[c], r_sl.at[c])
            wait_all(from_r.at[c], r_sr.at[c])
            total = partial[c, y].astype(F32) + from_l[c].astype(F32) + from_r[c].astype(F32)
            egrad[c] = total.astype(BF)
            for step in (4, 2, 6, 3, 5, 1, 7):
                peer, device = g_peer(step)
                send(
                    egrad.at[c, rows_of(peer)], recv_b2.at[c, rows_of(g)],
                    s_b2.at[c], r_b2.at[c], device,
                )
            recv_b2[c, rows_of(g), :] = egrad[c, rows_of(g), :]
        c = s - 2
        if 0 <= c < CH:
            wait_all(recv_b2.at[c, pl.ds(0, ROWS - BLOCK)], r_b2.at[c])
            out_a2[c] = nn(perm[...], recv_b2[c]).astype(BF)
            for step in (4, 3, 5, 2, 6, 1, 7):
                peer, device = z_peer(step)
                send(
                    out_a2.at[c, rows_of(peer)], coming.at[c, rows_of(z)],
                    s_a2.at[c], r_a2.at[c], device,
                )
            coming[c, rows_of(z), :] = out_a2[c, rows_of(z), :]
        c = s - 3
        if 0 <= c < CH:
            wait_all(coming.at[c, pl.ds(0, ROWS - BLOCK)], r_a2.at[c])
            summed = nn(sel_t[...], coming[c])
            mix[y, :, lanes(c)] = (cot[:, lanes(c)].astype(F32) + summed).astype(BF)
            mine = mix.at[y, :, lanes(c)]
            send(mine, mine, s_m.at[0, c], r_ml.at[c], to_right)
            send(mine, mine, s_m.at[1, c], r_mr.at[c], to_left)
        c = s - 4
        if 0 <= c < CH:
            size = coming.at[c, pl.ds(0, TOK)]
            wait_all(size, r_ml.at[c])
            passed = mix.at[left, pl.ds(0, TOK // 2), lanes(c)]
            send(passed, passed, s_m.at[2, c], r_nl.at[c], to_right)
            wait_all(size, r_mr.at[c])
            passed = mix.at[right, pl.ds(TOK // 2, TOK // 2), lanes(c)]
            send(passed, passed, s_m.at[3, c], r_nr.at[c], to_left)
        c = s - 5
        if 0 <= c < CH:
            size = coming.at[c, pl.ds(0, TOK // 2)]
            wait_all(size, r_nl.at[c])
            wait_all(size, r_nr.at[c])
        for _ in range(2):
            if work < 12:
                weight_grads(work)
                work += 1

    for c in range(CH):
        full, most, half = out_b.at[c], out_b.at[c, pl.ds(0, ROWS - BLOCK)], out_b.at[c, pl.ds(0, HALF)]
        for sem in (s_a, s_b, s_b2, s_a2):
            wait_all(most, sem.at[c])
        for i, size in enumerate((full, full, half, half)):
            wait_all(size, s_y.at[i, c])
        for i in range(6):
            wait_all(half, s_rs.at[i, c])
        for i in range(4):
            wait_all(out_b.at[c, pl.ds(0, TOK if i < 2 else TOK // 2)], s_m.at[i, c])


def moe(cot, route_ids, route_weight, rows_in, wg, wu, wd):
    at = jnp.arange(ROWS, dtype=jnp.int32)
    swapped = (at // CAP % NZ) * BLOCK + at // BLOCK * CAP + at % CAP
    perm = (swapped[:, None] == at[None, :]).astype(BF)
    ids = route_ids.astype(F32)
    vmem = pl.BlockSpec(memory_space=pltpu.VMEM)
    dma, V = pltpu.SemaphoreType.DMA, pltpu.VMEM
    chunked = V((CH, ROWS, LANES), BF)
    halves = V((CH, HALF, LANES), BF)
    return pl.pallas_call(
        moe_kernel,
        out_shape=(
            jax.ShapeDtypeStruct((2048, HID), BF),
            jax.ShapeDtypeStruct((2048, HID), BF),
            jax.ShapeDtypeStruct((HID, 2048), BF),
            jax.ShapeDtypeStruct((NY, TOK, WIDE), BF),
        ),
        in_specs=[vmem] * 9,
        out_specs=(vmem,) * 4,
        scratch_shapes=[
            chunked, chunked, chunked,
            V((NY, ROWS, WIDE), BF),
            V((ROWS, HID), BF), V((ROWS, HID), F32), V((ROWS, HID), F32), V((ROWS, HID), F32),
            V((ROWS, 2 * HID), BF), V((TOK, ROWS), BF), V((ROWS, 2048), BF),
            V((CH, NY, ROWS, LANES), BF),
            halves, halves, halves, halves,
            chunked, chunked, chunked, chunked, chunked, chunked,
            dma((CH,)), dma((CH,)), dma((CH,)), dma((CH,)),
            dma((4, CH)), dma((CH,)), dma((CH,)), dma((CH,)), dma((CH,)),
            dma((6, CH)), dma((CH,)), dma((CH,)), dma((CH,)), dma((CH,)),
            dma((CH,)), dma((CH,)), dma((CH,)), dma((CH,)),
            dma((4, CH)), dma((CH,)), dma((CH,)), dma((CH,)), dma((CH,)),
        ],
        compiler_params=pltpu.CompilerParams(
            collective_id=0, has_side_effects=True, vmem_limit_bytes=60 * 1024 * 1024
        ),
        name="moe",
    )(cot, ids, ids.T, route_weight.T, rows_in, wg, wu, wd, perm)


def in_blocks(value, dim, devices):
    dims = value.shape
    tiles = value.reshape(*dims[:dim], devices, dims[dim] // devices, *dims[dim + 1 :])
    return jnp.moveaxis(tiles, dim, 0)


def sum_at_owner(value, axis, dim):
    tiles = in_blocks(value, dim, lax.axis_size(axis))
    arrived = lax.all_to_all(tiles, axis, split_axis=0, concat_axis=0, tiled=True)
    return arrived.astype(jnp.float32).sum(axis=0)


def from_everyone(value, axis):
    devices = lax.axis_size(axis)
    return lax.all_to_all(
        jnp.broadcast_to(value[None], (devices, *value.shape)), axis, 0, 0, tiled=True
    )


def in_order(tiles, dim):
    dims = list(tiles.shape[1:])
    dims[dim] *= tiles.shape[0]
    return jnp.moveaxis(tiles, 0, dim).reshape(dims)


def collect(value, axis, dim):
    tiles = from_everyone(value, axis)
    return in_order(tiles, dim)


def sum_by_axis(subtotal, axes):
    for axis in axes:
        subtotal = lax.psum_scatter(subtotal, axis, scatter_dimension=0, tiled=True)
    return subtotal


def of_everyone(value, axis):
    return from_everyone(value, axis).sum(axis=0)


def in_one(arrays, axis):
    flat, at, done = (jnp.concatenate([a.reshape(-1) for a in arrays]), 0, [])
    subtotal = of_everyone(flat, axis)
    for a in arrays:
        done.append(subtotal[at : at + a.size].reshape(a.shape))
        at += a.size
    return tuple(done)


def passed_along(value, axis, steps):
    count = lax.axis_size(axis)
    leading, last = (max(0, -steps), min(count, count - steps))
    return lax.ppermute(value, axis, [(source, source + steps) for source in range(leading, last)])


def per_device(
    cot_out,
    route_ids,
    route_weight,
    expert_inputs,
    w_gate,
    w_up,
    w_down,
    w_proj,
    conv_out,
    channel_norm_gain,
    taps,
    value_pre,
    gate_pre,
):
    narrow_size = lax.axis_size("tp")
    tok_rows = cot_out.shape[0]
    local_cols = cot_out.shape[1]
    grad_gate_part, grad_up_part, grad_down, mix = moe(
        cot_out, route_ids, route_weight, expert_inputs[0], w_gate[0], w_up[0], w_down[0]
    )
    mix_full = jnp.transpose(mix, (1, 0, 2)).reshape(tok_rows, -1)
    convolution_filter = conv_out.astype(jnp.float32)
    channel_total = local_cols * narrow_size
    first_sum, square_sum = lax.psum(
        (
            jnp.sum(convolution_filter, axis=1),
            jnp.sum(convolution_filter * convolution_filter, axis=1),
        ),
        "tp",
    )
    channel_mean = (first_sum / channel_total)[:, None]
    var = (square_sum / channel_total)[:, None] - channel_mean * channel_mean
    inverse_deviation = lax.rsqrt(var + norm_epsilon)
    normalized_input = (convolution_filter - channel_mean) * inverse_deviation
    normalized_output = normalized_input * channel_norm_gain[None, :]
    sigma_conv = jax.nn.sigmoid(normalized_output)
    act_conv = (normalized_output * sigma_conv).astype(jnp.bfloat16)
    grad_proj = sum_by_axis(
        lax.dot_general(
            act_conv, mix_full, (((0,), (0,)), ((), ())), preferred_element_type=jnp.float32
        ),
        SP,
    )
    d_act_conv = jnp.dot(mix_full, w_proj.T, preferred_element_type=jnp.float32)
    normalized_gradient = (
        d_act_conv
        * sigma_conv
        * (1.0 + normalized_output * (1.0 - sigma_conv))
        * channel_norm_gain[None, :]
    )
    first_term_gradient, second_term_gradient = in_one(
        (
            jnp.sum(normalized_gradient, axis=1),
            jnp.sum(normalized_gradient * normalized_input, axis=1),
        ),
        "tp",
    )
    convolution_gradient = inverse_deviation * (
        normalized_gradient
        - (first_term_gradient / channel_total)[:, None]
        - normalized_input * (second_term_gradient / channel_total)[:, None]
    )
    reach = taps.shape[0]
    following = passed_along(convolution_gradient[: reach - 1], SP, -1)
    extended = jnp.concatenate([convolution_gradient, following], axis=0)
    d_glu = jnp.zeros_like(convolution_gradient)
    for offset in range(reach):
        begin = reach - 1 - offset
        d_glu = d_glu + taps[offset][None, :] * extended[begin : begin + tok_rows]
    gate_sig = jax.nn.sigmoid(gate_pre.astype(jnp.float32))
    grad_value = (d_glu * gate_sig).astype(jnp.bfloat16)
    grad_gate = (d_glu * value_pre.astype(jnp.float32) * gate_sig * (1.0 - gate_sig)).astype(
        jnp.bfloat16
    )
    return (
        grad_gate_part[None],
        grad_up_part[None],
        grad_down[None],
        grad_proj,
        grad_value,
        grad_gate,
    )


def solution(mesh):
    finer = Mesh(mesh.devices.reshape(8, 4, 2, mesh.shape["tp"]), ("sp_0", "sp_1", "sp_2", "tp"))
    placed = (
        P(SP, "tp"),
        P(SP, None),
        P(SP, None),
        P(SP, None, None),
        P(SP, None, "tp"),
        P(SP, None, "tp"),
        P(SP, "tp", None),
        P("tp", None),
        P(SP, "tp"),
        P("tp"),
        P(None, "tp"),
        P(SP, "tp"),
        P(SP, "tp"),
    )
    return jax.shard_map(
        per_device,
        mesh=finer,
        in_specs=placed,
        out_specs=(
            P(SP, None, "tp"),
            P(SP, None, "tp"),
            P(SP, "tp", None),
            P(TP_SP, None),
            P(SP, "tp"),
            P(SP, "tp"),
        ),
        check_vma=False,
    )
```

```python
import jax
import jax.numpy as jnp
from jax import lax
from jax.experimental import pallas as pl
from jax.experimental.pallas import tpu as pltpu
from jax.sharding import Mesh
from jax.sharding import PartitionSpec as P

SP = ("sp_0", "sp_1", "sp_2")
TP_SP = ("tp", "sp_0", "sp_1", "sp_2")
MESH = pl.DeviceIdType.MESH

clamp_limit = 7.0
swish_alpha = 1.702
norm_epsilon = 1e-05

CH = 4
LANES = 128
NZ = 8
NG = 8
NY = 4
CAP = 12
BLOCK = NZ * CAP
ROWS = NZ * BLOCK
HALF = ROWS // 2
TOK = 256
WIDE = CH * LANES
HID = 256
TAPS = 31
EXT = TOK + 32
CHANNELS = 2048
NX = 4
XROWS = 64
BF = jnp.bfloat16
F32 = jnp.float32


def nt(a, b):
    return lax.dot_general(a, b, (((1,), (1,)), ((), ())), preferred_element_type=F32)


def tn(a, b):
    return lax.dot_general(a, b, (((0,), (0,)), ((), ())), preferred_element_type=F32)


def nn(a, b):
    return lax.dot_general(a, b, (((1,), (0,)), ((), ())), preferred_element_type=F32)


def wait_all(ref, sem):
    pltpu.make_async_copy(ref, ref, sem).wait()


def send(src, dst, send_sem, recv_sem, device):
    pltpu.make_async_remote_copy(
        src_ref=src,
        dst_ref=dst,
        send_sem=send_sem,
        recv_sem=recv_sem,
        device_id=device,
        device_id_type=MESH,
    ).start()


def lanes(c):
    return pl.ds(c * LANES, LANES)


def rows_of(block):
    return pl.ds(pl.multiple_of(block * BLOCK, BLOCK), BLOCK)


def columns(parts, rows):
    lane = lax.broadcasted_iota(jnp.int32, (rows, LANES), 1)
    whole = jnp.zeros((rows, LANES), F32)
    for i, part in enumerate(parts):
        whole = jnp.where(lane == i, part, whole)
    return whole


def as_columns(rows8):
    return jnp.concatenate([rows8, jnp.zeros((LANES - 8, TOK), F32)], axis=0).T


def swap_matrix():
    at = lax.broadcasted_iota(jnp.int32, (ROWS, 1), 0).astype(F32)
    pair = jnp.floor((at + 0.5) * (1.0 / CAP))
    high = jnp.floor((pair + 0.5) * (1.0 / NZ))
    source = (pair - NZ * high) * BLOCK + high * CAP + (at - CAP * pair)
    lane = lax.broadcasted_iota(jnp.int32, (ROWS, ROWS), 1).astype(F32)
    return jnp.where(lane == source, 1.0, 0.0).astype(BF)


def step_kernel(
    cot, ids, route_w, conv, gain, taps, rows_hbm, wg_hbm, wu_hbm, wd_hbm, wp_hbm, value_hbm, gate_hbm,
    gg_hbm, gu_hbm, gd_hbm, gp_out, gv_out, gt_out,
    rows_in, wg, wu, wd, wp, value, gate, gg_out, gu_out, gd_out,
    perm, out_a, recv_a, out_b, cotf, act_s, f_up, f_gate, dact, dgu, sel_t, rows_p,
    partial, r1l, r1r, accl, accr, from_l, from_r, egrad, recv_b2, out_a2, coming, mix,
    stat, nstat, xhat, act_c, fac, rstd_s, sg, vg, dac, ext, halo,
    gpb, rc, gx, x1l, x1r, xal, xar, xfl, xfr, gz, rz,
    s_in, s_out,
    s_a, r_a, s_b, r_b, s_y, r_yl, r_yr, r_fl, r_fr,
    s_rs, r_1l, r_1r, r_sl, r_sr, s_b2, r_b2, s_a2, r_a2, s_m, r_ml, r_mr, r_nl, r_nr,
    s_stat, r_stat, s_n, r_n, s_h, r_h,
    s_c, r_c, s_x, r_x1l, r_x1r, r_xl, r_xr, s_z, r_z,
):
    z = lax.axis_index("sp_0")
    x = lax.axis_index("sp_1")
    core = lax.axis_index("sp_2")
    g = x * 2 + core
    y = lax.axis_index("tp")
    right, left, across = lax.rem(y + 1, NY), lax.rem(y + 3, NY), lax.rem(y + 2, NY)
    to_right, to_left, to_across = {"tp": right}, {"tp": left}, {"tp": across}
    x_right, x_left, x_across = lax.rem(x + 1, NX), lax.rem(x + 3, NX), lax.rem(x + 2, NX)
    to_x_right, to_x_left = {"sp_1": x_right}, {"sp_1": x_left}
    to_core = {"sp_2": 1 - core}
    place = z * NG + g

    def z_peer(step):
        peer = lax.rem(z + step, NZ)
        return peer, {"sp_0": peer}

    def g_peer(step):
        peer = lax.rem(g + step, NG)
        return peer, {"sp_1": peer // 2, "sp_2": lax.rem(peer, 2)}

    def in_line(step):
        other = lax.rem(place + step, NZ * NG)
        return {"sp_0": other // NG, "sp_1": lax.rem(other // 2, NX), "sp_2": lax.rem(other, 2)}

    to_before = in_line(NZ * NG - 1)
    barrier = pltpu.get_barrier_semaphore()
    greeted = [z_peer(step)[1] for step in range(1, NZ)] + [g_peer(step)[1] for step in range(1, NG)]
    greeted += [to_right, to_left, to_across, to_before, in_line(1)]
    for device in greeted:
        pl.semaphore_signal(barrier, inc=1, device_id=device, device_id_type=MESH)

    fetches = [
        pltpu.make_async_copy(src, dst, s_in.at[i])
        for i, (src, dst) in enumerate(
            ((rows_hbm, rows_in), (wg_hbm, wg), (wu_hbm, wu), (wd_hbm, wd),
             (gate_hbm, gate), (value_hbm, value), (wp_hbm, wp))
        )
    ]
    for fetch in fetches:
        fetch.start()

    t_sub = lax.broadcasted_iota(jnp.int32, (TOK, TOK), 0)
    t_lane = lax.broadcasted_iota(jnp.int32, (TOK, TOK), 1)
    before, after = t_sub < t_lane, t_lane < t_sub
    col = [ids[:, k : k + 1].astype(F32) for k in (0, 1)]
    turned = columns(col + [route_w[:, k : k + 1] for k in (0, 1)], TOK).T
    row = [turned[k : k + 1, :] for k in (0, 1)]
    w_r = [turned[k + 2 : k + 3, :] for k in (0, 1)]
    slot_r = lax.broadcasted_iota(jnp.int32, (ROWS, TOK), 0).astype(F32)
    chosen, weight = None, None
    for k in (0, 1):
        same = ((col[0] == row[k]) | (col[1] == row[k])) & before
        dest = jnp.sum(jnp.where(same, 1.0, 0.0), axis=0, keepdims=True) + CAP * row[k]
        hot = slot_r == dest
        one, scale = jnp.where(hot, 1.0, 0.0), jnp.where(hot, w_r[k], 0.0)
        chosen = one if chosen is None else chosen + one
        weight = scale if weight is None else weight + scale
    chosen = chosen.astype(BF)
    weight = jnp.sum(weight, axis=1, keepdims=True)

    for c in range(CH):
        out_a[c] = (weight * nn(chosen, cot[:, lanes(c)])).astype(BF)
        if c == 0:
            pl.semaphore_wait(barrier, len(greeted))
        for step in (4, 3, 5, 2, 6, 1, 7):
            peer, device = z_peer(step)
            send(out_a.at[c, rows_of(peer)], recv_a.at[c, rows_of(z)], s_a.at[c], r_a.at[c], device)
        recv_a[c, rows_of(z), :] = out_a[c, rows_of(z), :]

    wide = conv[...].astype(F32)
    sums = [jnp.sum(v, axis=1, keepdims=True) for v in (wide, wide * wide)]
    stat[y] = columns(sums, TOK).T[0:8, :]
    for i, device in enumerate((to_right, to_left, to_across)):
        send(stat.at[y], stat.at[y], s_stat.at[i], r_stat.at[0], device)

    perm[...] = swap_matrix()

    def unpack_slots():
        slot_c = lax.broadcasted_iota(jnp.int32, (TOK, ROWS), 1).astype(F32)
        back = None
        for k in (0, 1):
            same = ((row[0] == col[k]) | (row[1] == col[k])) & after
            dest = jnp.sum(jnp.where(same, 1.0, 0.0), axis=1, keepdims=True) + CAP * col[k]
            one = jnp.where(slot_c == dest, 1.0, 0.0)
            back = one if back is None else back + one
        sel_t[...] = back.astype(BF)

    def forward_rows():
        fetches[0].wait()
        for j in range(8):
            cols = pl.ds(j * 256, 256)
            rows_p[:, cols] = nn(perm[...], rows_in[:, cols]).astype(BF)
        fetches[1].wait()
        fetches[2].wait()
        fetches[3].wait()

    def forward_part(j):
        part = pl.ds(j * 256, 256)
        gate_lin = nn(rows_p[part, :], wg[...])
        up_lin = nn(rows_p[part, :], wu[...])
        gate_c = jnp.minimum(gate_lin, clamp_limit)
        up_c = jnp.clip(up_lin, -clamp_limit, clamp_limit)
        sig = jax.nn.sigmoid(swish_alpha * gate_c)
        act_s[part, :] = ((up_c + 1.0) * gate_c * sig).astype(BF)
        up_open = (up_lin > -clamp_limit) & (up_lin < clamp_limit)
        f_up[part, :] = jnp.where(up_open, gate_c * sig, 0.0)
        slope = (up_c + 1.0) * (sig + swish_alpha * gate_c * sig * (1.0 - sig))
        f_gate[part, :] = jnp.where(gate_lin < clamp_limit, slope, 0.0)

    def norm_terms():
        wait_all(stat.at[pl.ds(0, NY - 1)], r_stat.at[0])
        total = as_columns(stat[0] + stat[1] + stat[2] + stat[3])
        mean = total[:, 0:1] / CHANNELS
        var = total[:, 1:2] / CHANNELS - mean * mean
        rstd = lax.rsqrt(var + norm_epsilon)
        rstd_s[...] = rstd
        normalized = (conv[...].astype(F32) - mean) * rstd
        xhat[...] = normalized
        normed = normalized * gain[...]
        s = jax.nn.sigmoid(normed)
        act_c[...] = (normed * s).astype(BF)
        fac[...] = s * (1.0 + normed * (1.0 - s)) * gain[...]

    def glu_terms():
        fetches[4].wait()
        fetches[5].wait()
        gate_sig = jax.nn.sigmoid(gate[...].astype(F32))
        sg[...] = gate_sig
        vg[...] = value[...].astype(F32) * gate_sig * (1.0 - gate_sig)
        fetches[6].wait()

    fill = [unpack_slots, norm_terms, glu_terms]
    forward_rows()
    for j in range(3):
        forward_part(j)

    for s in range(CH + 3):
        c = s
        if 0 <= c < CH:
            wait_all(recv_a.at[c, pl.ds(0, ROWS - BLOCK)], r_a.at[c])
            out_b[c] = nn(perm[...], recv_a[c]).astype(BF)
            for step in (4, 2, 6, 3, 5, 1, 7):
                peer, device = g_peer(step)
                send(
                    out_b.at[c, rows_of(peer)], cotf.at[y, rows_of(g), lanes(c)],
                    s_b.at[c], r_b.at[c], device,
                )
            cotf[y, rows_of(g), lanes(c)] = out_b[c, rows_of(g), :]
        c = s - 1
        if 0 <= c < CH:
            wait_all(out_b.at[c, pl.ds(0, ROWS - BLOCK)], r_b.at[c])
            mine = cotf.at[y, :, lanes(c)]
            send(mine, mine, s_y.at[0, c], r_yl.at[c], to_right)
            send(mine, mine, s_y.at[1, c], r_yr.at[c], to_left)
        c = s - 2
        if 0 <= c < CH:
            wait_all(out_b.at[c], r_yl.at[c])
            passed = cotf.at[left, pl.ds(0, HALF), lanes(c)]
            send(passed, passed, s_y.at[2, c], r_fl.at[c], to_right)
            wait_all(out_b.at[c], r_yr.at[c])
            passed = cotf.at[right, pl.ds(HALF, HALF), lanes(c)]
            send(passed, passed, s_y.at[3, c], r_fr.at[c], to_left)
        c = s - 3
        if 0 <= c < CH:
            wait_all(out_b.at[c, pl.ds(0, HALF)], r_fl.at[c])
            wait_all(out_b.at[c, pl.ds(0, HALF)], r_fr.at[c])
            arrived = jnp.concatenate([cotf[q, :, lanes(c)] for q in range(NY)], axis=1)
            down = jnp.concatenate(
                [wd[:, pl.ds(q * WIDE + c * LANES, LANES)] for q in range(NY)], axis=1
            )
            term = nt(arrived, down)
            dact[...] = term if c == 0 else dact[...] + term
        if fill:
            fill.pop(0)()

    dgu[:, 0:HID] = (dact[...] * f_gate[...]).astype(BF)
    dgu[:, HID : 2 * HID] = (dact[...] * f_up[...]).astype(BF)

    for c in range(CH):
        weights = jnp.concatenate(
            [
                jnp.concatenate([w[pl.ds(q * WIDE + c * LANES, LANES), :] for w in (wg, wu)], axis=1)
                for q in range(NY)
            ],
            axis=0,
        )
        product = nt(dgu[...], weights).astype(BF)
        for q in range(NY):
            partial[c, q] = product[:, q * LANES : (q + 1) * LANES]
        low, high = pl.ds(0, HALF), pl.ds(HALF, HALF)
        send(partial.at[c, across, low], r1l.at[c], s_rs.at[0, c], r_1l.at[c], to_right)
        send(partial.at[c, across, high], r1r.at[c], s_rs.at[1, c], r_1r.at[c], to_left)
        send(partial.at[c, right, high], from_l.at[c, high], s_rs.at[2, c], r_sl.at[c], to_right)
        send(partial.at[c, left, low], from_r.at[c, low], s_rs.at[3, c], r_sr.at[c], to_left)

    def weight_grads(j):
        if j < 4:
            gd_out[:, pl.ds(j * WIDE, WIDE)] = tn(act_s[...], cotf[j]).astype(BF)
        else:
            part = pl.ds((j - 4) * 256, 256)
            both = tn(rows_p[:, part], dgu[...]).astype(BF)
            gg_out[part, :] = both[:, 0:HID]
            gu_out[part, :] = both[:, HID : 2 * HID]

    stores = [
        pltpu.make_async_copy(src, dst, s_out.at[i])
        for i, (src, dst) in enumerate(((gg_out, gg_hbm), (gu_out, gu_hbm), (gd_out, gd_hbm)))
    ]

    def norm_grad_sums():
        grad = dac[...] * fac[...]
        dac[...] = grad
        sums = [jnp.sum(v, axis=1, keepdims=True) for v in (grad, grad * xhat[...])]
        nstat[y] = columns(sums, TOK).T[0:8, :]
        for i, device in enumerate((to_right, to_left, to_across)):
            send(nstat.at[y], nstat.at[y], s_n.at[i], r_n.at[0], device)

    def conv_grad():
        wait_all(nstat.at[pl.ds(0, NY - 1)], r_n.at[0])
        total = as_columns(nstat[0] + nstat[1] + nstat[2] + nstat[3]) / CHANNELS
        ext[0:TOK, :] = rstd_s[...] * (dac[...] - total[:, 0:1] - xhat[...] * total[:, 1:2])
        send(ext.at[pl.ds(0, 32)], halo, s_h.at[0], r_h.at[0], to_before)

    def conv_rows(begin):
        part = pl.ds(begin, TOK // 2)

        def column(j, carry):
            cols = pl.ds(pl.multiple_of(j * LANES, LANES), LANES)
            total = jnp.zeros((TOK // 2, LANES), F32)
            for k in range(TAPS):
                total = total + taps[k : k + 1, cols] * ext[pl.ds(begin + TAPS - 1 - k, TOK // 2), cols]
            gv_out[part, cols] = (total * sg[part, cols]).astype(BF)
            gt_out[part, cols] = (total * vg[part, cols]).astype(BF)
            return carry

        lax.fori_loop(0, CH, column, 0)

    def conv_first():
        conv_rows(0)

    def conv_rest():
        wait_all(halo, r_h.at[0])
        keep = jnp.where(place == NZ * NG - 1, 0.0, 1.0)
        ext[TOK:EXT, :] = halo[...] * keep
        conv_rows(TOK // 2)

    work = 0
    for s in range(CH + 9):
        c = s
        if 0 <= c < CH:
            low, high = pl.ds(0, HALF), pl.ds(HALF, HALF)
            wait_all(r1l.at[c], r_1l.at[c])
            accr[c] = (partial[c, right, low, :].astype(F32) + r1l[c].astype(F32)).astype(BF)
            send(accr.at[c], from_l.at[c, low], s_rs.at[4, c], r_sl.at[c], to_right)
            wait_all(r1r.at[c], r_1r.at[c])
            accl[c] = (partial[c, left, high, :].astype(F32) + r1r[c].astype(F32)).astype(BF)
            send(accl.at[c], from_r.at[c, high], s_rs.at[5, c], r_sr.at[c], to_left)
        c = s - 1
        if 0 <= c < CH:
            wait_all(from_l.at[c], r_sl.at[c])
            wait_all(from_r.at[c], r_sr.at[c])
            total = partial[c, y].astype(F32) + from_l[c].astype(F32) + from_r[c].astype(F32)
            egrad[c] = total.astype(BF)
            for step in (4, 2, 6, 3, 5, 1, 7):
                peer, device = g_peer(step)
                send(
                    egrad.at[c, rows_of(peer)], recv_b2.at[c, rows_of(g)],
                    s_b2.at[c], r_b2.at[c], device,
                )
            recv_b2[c, rows_of(g), :] = egrad[c, rows_of(g), :]
        c = s - 2
        if 0 <= c < CH:
            wait_all(recv_b2.at[c, pl.ds(0, ROWS - BLOCK)], r_b2.at[c])
            out_a2[c] = nn(perm[...], recv_b2[c]).astype(BF)
            for step in (4, 3, 5, 2, 6, 1, 7):
                peer, device = z_peer(step)
                send(
                    out_a2.at[c, rows_of(peer)], coming.at[c, rows_of(z)],
                    s_a2.at[c], r_a2.at[c], device,
                )
            coming[c, rows_of(z), :] = out_a2[c, rows_of(z), :]
        c = s - 3
        if 0 <= c < CH:
            wait_all(coming.at[c, pl.ds(0, ROWS - BLOCK)], r_a2.at[c])
            summed = nn(sel_t[...], coming[c])
            mix[y, :, lanes(c)] = (cot[:, lanes(c)].astype(F32) + summed).astype(BF)
            mine = mix.at[y, :, lanes(c)]
            send(mine, mine, s_m.at[0, c], r_ml.at[c], to_right)
            send(mine, mine, s_m.at[1, c], r_mr.at[c], to_left)
        c = s - 4
        if 0 <= c < CH:
            size = coming.at[c, pl.ds(0, TOK)]
            wait_all(size, r_ml.at[c])
            passed = mix.at[left, pl.ds(0, TOK // 2), lanes(c)]
            send(passed, passed, s_m.at[2, c], r_nl.at[c], to_right)
            wait_all(size, r_mr.at[c])
            passed = mix.at[right, pl.ds(TOK // 2, TOK // 2), lanes(c)]
            send(passed, passed, s_m.at[3, c], r_nr.at[c], to_left)
        c = s - 5
        if 0 <= c < CH:
            size = coming.at[c, pl.ds(0, TOK // 2)]
            wait_all(size, r_nl.at[c])
            wait_all(size, r_nr.at[c])
            arrived = jnp.concatenate([mix[q, :, lanes(c)] for q in range(NY)], axis=1)
            proj = jnp.concatenate(
                [wp[:, pl.ds(q * WIDE + c * LANES, LANES)] for q in range(NY)], axis=1
            )
            term = nt(arrived, proj)
            dac[...] = term if c == 0 else dac[...] + term
            if c == CH - 1:
                norm_grad_sums()
            product = tn(act_c[...], arrived)
            for core_at in range(2):
                for x_at in range(NX):
                    gpb[c, core_at, x_at] = jnp.concatenate(
                        [
                            product[(z_at * NG + x_at * 2 + core_at) * 8 :][:8]
                            for z_at in range(NZ)
                        ],
                        axis=0,
                    ).astype(BF)
            send(gpb.at[c, 1 - core], rc.at[c], s_c.at[c], r_c.at[c], to_core)
        c = s - 6
        if 0 <= c < CH:
            wait_all(rc.at[c], r_c.at[c])
            gx[c] = (gpb[c, core].astype(F32) + rc[c].astype(F32)).astype(BF)
            low, high = pl.ds(0, XROWS // 2), pl.ds(XROWS // 2, XROWS // 2)
            send(gx.at[c, x_across, low], x1l.at[c], s_x.at[0, c], r_x1l.at[c], to_x_right)
            send(gx.at[c, x_across, high], x1r.at[c], s_x.at[1, c], r_x1r.at[c], to_x_left)
            send(gx.at[c, x_right, high], xfl.at[c, high], s_x.at[2, c], r_xl.at[c], to_x_right)
            send(gx.at[c, x_left, low], xfr.at[c, low], s_x.at[3, c], r_xr.at[c], to_x_left)
        c = s - 7
        if 0 <= c < CH:
            low, high = pl.ds(0, XROWS // 2), pl.ds(XROWS // 2, XROWS // 2)
            wait_all(x1l.at[c], r_x1l.at[c])
            xar[c] = (gx[c, x_right, low, :].astype(F32) + x1l[c].astype(F32)).astype(BF)
            send(xar.at[c], xfl.at[c, low], s_x.at[4, c], r_xl.at[c], to_x_right)
            wait_all(x1r.at[c], r_x1r.at[c])
            xal[c] = (gx[c, x_left, high, :].astype(F32) + x1r[c].astype(F32)).astype(BF)
            send(xal.at[c], xfr.at[c, high], s_x.at[5, c], r_xr.at[c], to_x_left)
            if c == CH - 2:
                conv_grad()
        c = s - 8
        if 0 <= c < CH:
            wait_all(xfl.at[c], r_xl.at[c])
            wait_all(xfr.at[c], r_xr.at[c])
            total = gx[c, x].astype(F32) + xfl[c].astype(F32) + xfr[c].astype(F32)
            gz[c] = jnp.concatenate(
                [
                    total[z_at * 8 : z_at * 8 + 8, half * 256 : half * 256 + 256]
                    for z_at in range(NZ)
                    for half in (0, 1)
                ],
                axis=0,
            ).astype(BF)
            for step in (4, 3, 5, 2, 6, 1, 7):
                peer, device = z_peer(step)
                send(
                    gz.at[c, pl.ds(pl.multiple_of(peer * 16, 16), 16)],
                    rz.at[c, pl.ds(pl.multiple_of(z * 16, 16), 16)],
                    s_z.at[c], r_z.at[c], device,
                )
            own = pl.ds(pl.multiple_of(z * 16, 16), 16)
            rz[c, own, :] = gz[c, own, :]
            if c == CH - 2:
                conv_first()
            if c == CH - 1:
                conv_rest()
        for _ in range(2):
            if work < 12:
                weight_grads(work)
                work += 1
                if work == 4:
                    stores[2].start()
                if work == 12:
                    stores[0].start()
                    stores[1].start()

    for c in range(CH):
        wait_all(rz.at[c, pl.ds(0, 112)], r_z.at[c])
        total = rz[c, 0:16, :].astype(F32)
        for z_at in range(1, NZ):
            total = total + rz[c, z_at * 16 : z_at * 16 + 16, :].astype(F32)
        for q in range(NY):
            row_at, lane_at = (q // 2) * 8, (q % 2) * LANES
            gp_out[:, pl.ds(q * WIDE + c * LANES, LANES)] = total[
                row_at : row_at + 8, lane_at : lane_at + LANES
            ]

    for c in range(CH):
        full, most, half = out_b.at[c], out_b.at[c, pl.ds(0, ROWS - BLOCK)], out_b.at[c, pl.ds(0, HALF)]
        for sem in (s_a, s_b, s_b2, s_a2):
            wait_all(most, sem.at[c])
        for i, size in enumerate((full, full, half, half)):
            wait_all(size, s_y.at[i, c])
        for i in range(6):
            wait_all(half, s_rs.at[i, c])
        for i in range(4):
            wait_all(out_b.at[c, pl.ds(0, TOK if i < 2 else TOK // 2)], s_m.at[i, c])
        wait_all(rc.at[c], s_c.at[c])
        for i in range(6):
            wait_all(x1l.at[c], s_x.at[i, c])
        wait_all(rz.at[c, pl.ds(0, 112)], s_z.at[c])
    for i in range(3):
        wait_all(stat.at[0], s_stat.at[i])
        wait_all(nstat.at[0], s_n.at[i])
        stores[i].wait()
    wait_all(halo, s_h.at[0])


def per_device(
    cot_out,
    route_ids,
    route_weight,
    expert_inputs,
    w_gate,
    w_up,
    w_down,
    w_proj,
    conv_out,
    channel_norm_gain,
    taps,
    value_pre,
    gate_pre,
):
    vmem = pl.BlockSpec(memory_space=pltpu.VMEM)
    anywhere = pl.BlockSpec(memory_space=pl.ANY)
    dma, V = pltpu.SemaphoreType.DMA, pltpu.VMEM
    chunked = V((CH, ROWS, LANES), BF)
    halves = V((CH, HALF, LANES), BF)
    tokens = V((TOK, WIDE), F32)
    x_half = V((CH, XROWS // 2, WIDE), BF)
    per_chunk = dma((CH,))
    gate_grad, up_grad, down_grad, proj_grad, grad_value, grad_gate = pl.pallas_call(
        step_kernel,
        out_shape=(
            jax.ShapeDtypeStruct((CHANNELS, HID), BF),
            jax.ShapeDtypeStruct((CHANNELS, HID), BF),
            jax.ShapeDtypeStruct((HID, CHANNELS), BF),
            jax.ShapeDtypeStruct((8, CHANNELS), F32),
            jax.ShapeDtypeStruct((TOK, WIDE), BF),
            jax.ShapeDtypeStruct((TOK, WIDE), BF),
        ),
        in_specs=[vmem] * 6 + [anywhere] * 7,
        out_specs=(anywhere,) * 3 + (vmem,) * 3,
        scratch_shapes=[
            V((ROWS, CHANNELS), BF), V((CHANNELS, HID), BF), V((CHANNELS, HID), BF),
            V((HID, CHANNELS), BF), V((WIDE, CHANNELS), BF), V((TOK, WIDE), BF), V((TOK, WIDE), BF),
            V((CHANNELS, HID), BF), V((CHANNELS, HID), BF), V((HID, CHANNELS), BF),
            V((ROWS, ROWS), BF),
            chunked, chunked, chunked,
            V((NY, ROWS, WIDE), BF),
            V((ROWS, HID), BF), V((ROWS, HID), F32), V((ROWS, HID), F32), V((ROWS, HID), F32),
            V((ROWS, 2 * HID), BF), V((TOK, ROWS), BF), V((ROWS, CHANNELS), BF),
            V((CH, NY, ROWS, LANES), BF),
            halves, halves, halves, halves,
            chunked, chunked, chunked, chunked, chunked, chunked,
            V((NY, TOK, WIDE), BF),
            V((NY, 8, TOK), F32), V((NY, 8, TOK), F32),
            tokens, V((TOK, WIDE), BF), tokens, V((TOK, 1), F32), tokens, tokens, tokens,
            V((EXT, WIDE), F32), V((32, WIDE), F32),
            V((CH, 2, NX, XROWS, WIDE), BF), V((CH, NX, XROWS, WIDE), BF),
            V((CH, NX, XROWS, WIDE), BF),
            x_half, x_half, x_half, x_half,
            V((CH, XROWS, WIDE), BF), V((CH, XROWS, WIDE), BF),
            V((CH, 2 * XROWS, WIDE // 2), BF), V((CH, 2 * XROWS, WIDE // 2), BF),
            dma((7,)), dma((3,)),
            per_chunk, per_chunk, per_chunk, per_chunk,
            dma((4, CH)), per_chunk, per_chunk, per_chunk, per_chunk,
            dma((6, CH)), per_chunk, per_chunk, per_chunk, per_chunk,
            per_chunk, per_chunk, per_chunk, per_chunk,
            dma((4, CH)), per_chunk, per_chunk, per_chunk, per_chunk,
            dma((3,)), dma((1,)), dma((3,)), dma((1,)), dma((1,)), dma((1,)),
            per_chunk, per_chunk, dma((6, CH)), per_chunk, per_chunk, per_chunk, per_chunk,
            per_chunk, per_chunk,
        ],
        compiler_params=pltpu.CompilerParams(
            collective_id=0, has_side_effects=True, vmem_limit_bytes=62 * 1024 * 1024
        ),
        name="step",
    )(
        cot_out, route_ids, route_weight, conv_out, channel_norm_gain[None, :], taps,
        expert_inputs[0], w_gate[0], w_up[0], w_down[0], w_proj, value_pre, gate_pre,
    )
    return gate_grad[None], up_grad[None], down_grad[None], proj_grad, grad_value, grad_gate


def solution(mesh):
    finer = Mesh(mesh.devices.reshape(8, 4, 2, mesh.shape["tp"]), ("sp_0", "sp_1", "sp_2", "tp"))
    placed = (
        P(SP, "tp"),
        P(SP, None),
        P(SP, None),
        P(SP, None, None),
        P(SP, None, "tp"),
        P(SP, None, "tp"),
        P(SP, "tp", None),
        P("tp", None),
        P(SP, "tp"),
        P("tp"),
        P(None, "tp"),
        P(SP, "tp"),
        P(SP, "tp"),
    )
    return jax.shard_map(
        per_device,
        mesh=finer,
        in_specs=placed,
        out_specs=(
            P(SP, None, "tp"),
            P(SP, None, "tp"),
            P(SP, "tp", None),
            P(TP_SP, None),
            P(SP, "tp"),
            P(SP, "tp"),
        ),
        check_vma=False,
    )
```

```python
import functools

import jax
import jax.numpy as jnp
from jax import lax
from jax.experimental import pallas as pl
from jax.experimental.pallas import tpu as pltpu
from jax.sharding import Mesh
from jax.sharding import PartitionSpec as P

SP = ("sp_0", "sp_1", "sp_2")
TP_SP = ("tp", "sp_0", "sp_1", "sp_2")
MESH = pl.DeviceIdType.MESH

clamp_limit = 7.0
swish_alpha = 1.702
norm_epsilon = 1e-05

CH = 4
LANES = 128
NZ = 8
NG = 8
NY = 4
CAP = 12
HALVES = 2
SUB = CAP // HALVES
STEPS = HALVES * CH
BLOCK = NZ * SUB
PART = NZ * BLOCK
ROWS = HALVES * PART
HALF = PART // 2
MOST = PART - BLOCK
TOK = 256
WIDE = CH * LANES
HID = 256
TAPS = 31
FIRST_FILL = 8
DISPATCH = (
    "Z0", "Z1", "G0", "Z2", "G1", "Z3", "G2", "Y0", "Z4", "G3", "Y1", "D0", "Z5", "G4", "Y2",
    "D1", "Z6", "G5", "Y3", "D2", "Z7", "G6", "Y4", "G7", "D3", "I0",
)
BETWEEN = (
    "Y5", "D4", "P0", "Y6", "D5", "P1", "Y7", "D6", "P2", "D7", "I1",
)
RETURN = (
    "P3", "W0", "W1", "W2", "W3", "P4", "B0", "B1", "P5", "B2", "B3", "P6", "W4", "P7", "W5",
    "B4", "W6", "B5", "W7", "B6", "T0", "T1", "T2", "T3", "T4", "B7", "T5", "M0", "T6", "M1",
    "X0", "T7", "M2", "X1", "C0", "M3", "X2", "C1", "X3", "K0", "C2", "K1", "L0", "C3", "K2",
    "L1", "K3", "L2", "L3",
)
EXT = TOK + 32
CHANNELS = 2048
NX = 4
XROWS = 64
BF = jnp.bfloat16
F32 = jnp.float32


def nt(a, b):
    return lax.dot_general(a, b, (((1,), (1,)), ((), ())), preferred_element_type=F32)


def tn(a, b):
    return lax.dot_general(a, b, (((0,), (0,)), ((), ())), preferred_element_type=F32)


def nn(a, b):
    return lax.dot_general(a, b, (((1,), (0,)), ((), ())), preferred_element_type=F32)


def wait_all(ref, sem):
    pltpu.make_async_copy(ref, ref, sem).wait()


def send(src, dst, send_sem, recv_sem, device):
    pltpu.make_async_remote_copy(
        src_ref=src,
        dst_ref=dst,
        send_sem=send_sem,
        recv_sem=recv_sem,
        device_id=device,
        device_id_type=MESH,
    ).start()


def lanes(c):
    return pl.ds(c * LANES, LANES)


def rows_of(block):
    return pl.ds(pl.multiple_of(block * BLOCK, BLOCK), BLOCK)


def columns(parts, rows):
    lane = lax.broadcasted_iota(jnp.int32, (rows, LANES), 1)
    whole = jnp.zeros((rows, LANES), F32)
    for i, part in enumerate(parts):
        whole = jnp.where(lane == i, part, whole)
    return whole


def as_columns(rows8):
    return jnp.concatenate([rows8, jnp.zeros((LANES - 8, TOK), F32)], axis=0).T


def digits(at, low, high):
    rest = jnp.floor((at + 0.5) * (1.0 / low))
    top = jnp.floor((rest + 0.5) * (1.0 / high))
    return top, rest - high * top, at - low * rest


def hot_rows(source, count):
    lane = lax.broadcasted_iota(jnp.int32, (source.shape[0], count), 1).astype(F32)
    return jnp.where(lane == source, 1.0, 0.0).astype(BF)


def swap_matrix():
    at = lax.broadcasted_iota(jnp.int32, (PART, 1), 0).astype(F32)
    b, a, slot = digits(at, SUB, NZ)
    return hot_rows(a * BLOCK + b * SUB + slot, PART)


def order_matrix(half):
    at = lax.broadcasted_iota(jnp.int32, (PART, 1), 0).astype(F32)
    g, z, slot = digits(at, SUB, NZ)
    return hot_rows((z * NG + g) * CAP + half * SUB + slot, ROWS)


def step_kernel(
    cot, ids, route_w, conv, gain, taps, rows_hbm, wg_hbm, wu_hbm, wd_hbm, wp_hbm, value_hbm, gate_hbm,
    gg_hbm, gu_hbm, gd_hbm, gp_out, gv_out, gt_out,
    rows_in, wg, wu, wd, wp, value, gate, gg_out, gu_out, gd_out,
    perm, order, out_a, recv_a, out_b, cotf, act_s, f_up, f_gate, dact, up_rest, dgu, sel_t, rows_p,
    partial, r1l, r1r, accl, accr, from_l, from_r, egrad, recv_b2, out_a2, coming, mix,
    stat, nstat, xhat, act_c, fac, rstd_s, sg, vg, dac, ext, halo,
    gpb, rc, gx, x1l, x1r, xal, xar, xfl, xfr, gz, rz,
    s_in, s_out,
    s_a, r_a, s_b, r_b, s_y, r_yl, r_yr, r_fl, r_fr,
    s_rs, r_1l, r_1r, r_sl, r_sr, s_b2, r_b2, s_a2, r_a2, s_m, r_ml, r_mr, r_nl, r_nr,
    s_stat, r_stat, s_n, r_n, s_h, r_h,
    s_c, r_c, s_x, r_x1l, r_x1r, r_xl, r_xr, s_z, r_z,
):
    z = lax.axis_index("sp_0")
    x = lax.axis_index("sp_1")
    core = lax.axis_index("sp_2")
    g = x * 2 + core
    y = lax.axis_index("tp")
    right, left, across = lax.rem(y + 1, NY), lax.rem(y + 3, NY), lax.rem(y + 2, NY)
    to_right, to_left, to_across = {"tp": right}, {"tp": left}, {"tp": across}
    x_right, x_left, x_across = lax.rem(x + 1, NX), lax.rem(x + 3, NX), lax.rem(x + 2, NX)
    to_x_right, to_x_left = {"sp_1": x_right}, {"sp_1": x_left}
    to_core = {"sp_2": 1 - core}
    place = z * NG + g

    def z_peer(step):
        peer = lax.rem(z + step, NZ)
        return peer, {"sp_0": peer}

    def g_peer(step):
        peer = lax.rem(g + step, NG)
        return peer, {"sp_1": peer // 2, "sp_2": lax.rem(peer, 2)}

    def in_line(step):
        other = lax.rem(place + step, NZ * NG)
        return {"sp_0": other // NG, "sp_1": lax.rem(other // 2, NX), "sp_2": lax.rem(other, 2)}

    to_before = in_line(NZ * NG - 1)
    barrier = pltpu.get_barrier_semaphore()
    greeted = [z_peer(step)[1] for step in range(1, NZ)] + [g_peer(step)[1] for step in range(1, NG)]
    greeted += [to_right, to_left, to_across, to_before, in_line(1)]
    for device in greeted:
        pl.semaphore_signal(barrier, inc=1, device_id=device, device_id_type=MESH)

    fetches = [
        pltpu.make_async_copy(src, dst, s_in.at[i])
        for i, (src, dst) in enumerate(
            ((rows_hbm, rows_in), (wg_hbm, wg), (wu_hbm, wu), (wd_hbm, wd),
             (gate_hbm, gate), (value_hbm, value), (wp_hbm, wp))
        )
    ]
    for fetch in fetches:
        fetch.start()

    t_sub = lax.broadcasted_iota(jnp.int32, (TOK, TOK), 0)
    t_lane = lax.broadcasted_iota(jnp.int32, (TOK, TOK), 1)
    before, after = t_sub < t_lane, t_lane < t_sub
    row = [ids[k : k + 1, :].astype(F32) for k in (0, 1)]
    w_r = [route_w[k : k + 1, :] for k in (0, 1)]
    turned = as_columns(jnp.concatenate(row + [jnp.zeros((6, TOK), F32)], axis=0))
    col = [turned[:, k : k + 1] for k in (0, 1)]

    def row_of(slot, expert):
        return slot + SUB * expert + jnp.where(slot >= SUB, 1.0 * (PART - SUB), 0.0)

    slot_r = lax.broadcasted_iota(jnp.int32, (ROWS, TOK), 0).astype(F32)
    chosen, weight = None, None
    for k in (0, 1):
        same = ((col[0] == row[k]) | (col[1] == row[k])) & before
        dest = row_of(jnp.sum(jnp.where(same, 1.0, 0.0), axis=0, keepdims=True), row[k])
        hot = slot_r == dest
        one, scale = jnp.where(hot, 1.0, 0.0), jnp.where(hot, w_r[k], 0.0)
        chosen = one if chosen is None else chosen + one
        weight = scale if weight is None else weight + scale
    chosen = chosen.astype(BF)
    weight = jnp.sum(weight, axis=1, keepdims=True)

    for i in range(STEPS):
        c, part = i % CH, slice(i // CH * PART, i // CH * PART + PART)
        out_a[i] = (weight[part] * nn(chosen[part], cot[:, lanes(c)])).astype(BF)
        if i == 0:
            pl.semaphore_wait(barrier, len(greeted))
        for step in (4, 3, 5, 2, 6, 1, 7):
            peer, device = z_peer(step)
            send(out_a.at[i, rows_of(peer)], recv_a.at[i, rows_of(z)], s_a.at[i], r_a.at[i], device)
        recv_a[i, rows_of(z), :] = out_a[i, rows_of(z), :]

    wide = conv[...].astype(F32)
    sums = [jnp.sum(v, axis=1, keepdims=True) for v in (wide, wide * wide)]
    stat[y] = columns(sums, TOK).T[0:8, :]
    for i, device in enumerate((to_right, to_left, to_across)):
        send(stat.at[y], stat.at[y], s_stat.at[i], r_stat.at[0], device)

    perm[...] = swap_matrix()

    def unpack_slots():
        slot_c = lax.broadcasted_iota(jnp.int32, (TOK, ROWS), 1).astype(F32)
        back = None
        for k in (0, 1):
            same = ((row[0] == col[k]) | (row[1] == col[k])) & after
            dest = row_of(jnp.sum(jnp.where(same, 1.0, 0.0), axis=1, keepdims=True), col[k])
            one = jnp.where(slot_c == dest, 1.0, 0.0)
            back = one if back is None else back + one
        sel_t[...] = back.astype(BF)

    def forward_rows(half, j):
        if j == 0:
            if half == 0:
                fetches[0].wait()
            order[...] = order_matrix(half)
        cols = pl.ds(j * 512, 512)
        rows_p[pl.ds(half * PART, PART), cols] = nn(order[...], rows_in[:, cols]).astype(BF)

    def forward_sums(j):
        total, w = ((f_gate, wg), (f_up, wu), (dact, wg), (up_rest, wu))[j]
        if j < 2:
            fetches[j + 1].wait()
        half = pl.ds(j // 2 * (CHANNELS // 2), CHANNELS // 2)
        total[...] = nn(rows_p[:, half], w[half, :])

    def forward_part(j):
        part = pl.ds(j * 256, 256)
        gate_lin = f_gate[part, :] + dact[part, :]
        up_lin = f_up[part, :] + up_rest[part, :]
        gate_c = jnp.minimum(gate_lin, clamp_limit)
        up_c = jnp.clip(up_lin, -clamp_limit, clamp_limit)
        sig = jax.nn.sigmoid(swish_alpha * gate_c)
        act_s[part, :] = ((up_c + 1.0) * gate_c * sig).astype(BF)
        up_open = (up_lin > -clamp_limit) & (up_lin < clamp_limit)
        f_up[part, :] = jnp.where(up_open, gate_c * sig, 0.0)
        slope = (up_c + 1.0) * (sig + swish_alpha * gate_c * sig * (1.0 - sig))
        f_gate[part, :] = jnp.where(gate_lin < clamp_limit, slope, 0.0)

    def norm_terms():
        wait_all(stat.at[pl.ds(0, NY - 1)], r_stat.at[0])
        total = as_columns(stat[0] + stat[1] + stat[2] + stat[3])
        mean = total[:, 0:1] / CHANNELS
        var = total[:, 1:2] / CHANNELS - mean * mean
        rstd = lax.rsqrt(var + norm_epsilon)
        rstd_s[...] = rstd
        normalized = (conv[...].astype(F32) - mean) * rstd
        xhat[...] = normalized
        normed = normalized * gain[...]
        s = jax.nn.sigmoid(normed)
        act_c[...] = (normed * s).astype(BF)
        fac[...] = s * (1.0 + normed * (1.0 - s)) * gain[...]

    def glu_terms():
        fetches[4].wait()
        fetches[5].wait()
        gate_sig = jax.nn.sigmoid(gate[...].astype(F32))
        sg[...] = gate_sig
        vg[...] = value[...].astype(F32) * gate_sig * (1.0 - gate_sig)
        fetches[6].wait()

    fill = [functools.partial(forward_rows, half, j) for half in range(HALVES) for j in range(4)]
    fill += [functools.partial(forward_sums, j) for j in range(4)]
    fill += [functools.partial(forward_part, j) for j in range(3)]
    fill += [fetches[3].wait, norm_terms, unpack_slots, glu_terms]
    for _ in range(FIRST_FILL):
        fill.pop(0)()

    def rows_at(i):
        return pl.ds(i // CH * PART, PART)

    def half_at(i, which):
        return pl.ds(i // CH * PART + which * HALF, HALF)

    low, high = pl.ds(0, HALF), pl.ds(HALF, HALF)

    def from_z(i):
        wait_all(recv_a.at[i, pl.ds(0, MOST)], r_a.at[i])
        out_b[i] = nn(perm[...], recv_a[i]).astype(BF)
        mine = pl.ds(pl.multiple_of(i // CH * PART + g * BLOCK, BLOCK), BLOCK)
        for step in (4, 2, 6, 3, 5, 1, 7):
            peer, device = g_peer(step)
            send(
                out_b.at[i, rows_of(peer)], cotf.at[y, mine, lanes(i % CH)],
                s_b.at[i], r_b.at[i], device,
            )
        cotf[y, mine, lanes(i % CH)] = out_b[i, rows_of(g), :]

    def from_g(i):
        wait_all(out_b.at[i, pl.ds(0, MOST)], r_b.at[i])
        mine = cotf.at[y, rows_at(i), lanes(i % CH)]
        send(mine, mine, s_y.at[0, i], r_yl.at[i], to_right)
        send(mine, mine, s_y.at[1, i], r_yr.at[i], to_left)

    def from_y(i):
        wait_all(out_b.at[i], r_yl.at[i])
        passed = cotf.at[left, half_at(i, 0), lanes(i % CH)]
        send(passed, passed, s_y.at[2, i], r_fl.at[i], to_right)
        wait_all(out_b.at[i], r_yr.at[i])
        passed = cotf.at[right, half_at(i, 1), lanes(i % CH)]
        send(passed, passed, s_y.at[3, i], r_fr.at[i], to_left)

    def gathered(i):
        c, part = i % CH, rows_at(i)
        wait_all(out_b.at[i, low], r_fl.at[i])
        wait_all(out_b.at[i, low], r_fr.at[i])
        arrived = jnp.concatenate([cotf[q, part, lanes(c)] for q in range(NY)], axis=1)
        down = jnp.concatenate(
            [wd[:, pl.ds(q * WIDE + c * LANES, LANES)] for q in range(NY)], axis=1
        )
        term = nt(arrived, down)
        dact[part, :] = term if c == 0 else dact[part, :] + term

    def input_grads(half):
        part = pl.ds(half * PART, PART)
        dgu[part, 0:HID] = (dact[part, :] * f_gate[part, :]).astype(BF)
        dgu[part, HID : 2 * HID] = (dact[part, :] * f_up[part, :]).astype(BF)
        for c in range(CH):
            i = half * CH + c
            weights = jnp.concatenate(
                [
                    jnp.concatenate(
                        [w[pl.ds(q * WIDE + c * LANES, LANES), :] for w in (wg, wu)], axis=1
                    )
                    for q in range(NY)
                ],
                axis=0,
            )
            product = nt(dgu[part, :], weights).astype(BF)
            for q in range(NY):
                partial[i, q] = product[:, q * LANES : (q + 1) * LANES]
            send(partial.at[i, across, low], r1l.at[i], s_rs.at[0, i], r_1l.at[i], to_right)
            send(partial.at[i, across, high], r1r.at[i], s_rs.at[1, i], r_1r.at[i], to_left)
            send(partial.at[i, right, high], from_l.at[i, high], s_rs.at[2, i], r_sl.at[i], to_right)
            send(partial.at[i, left, low], from_r.at[i, low], s_rs.at[3, i], r_sr.at[i], to_left)

    def partial_sums(i):
        wait_all(r1l.at[i], r_1l.at[i])
        accr[i] = (partial[i, right, low, :].astype(F32) + r1l[i].astype(F32)).astype(BF)
        send(accr.at[i], from_l.at[i, low], s_rs.at[4, i], r_sl.at[i], to_right)
        wait_all(r1r.at[i], r_1r.at[i])
        accl[i] = (partial[i, left, high, :].astype(F32) + r1r[i].astype(F32)).astype(BF)
        send(accl.at[i], from_r.at[i, high], s_rs.at[5, i], r_sr.at[i], to_left)

    def whole_sums(i):
        wait_all(from_l.at[i], r_sl.at[i])
        wait_all(from_r.at[i], r_sr.at[i])
        total = partial[i, y].astype(F32) + from_l[i].astype(F32) + from_r[i].astype(F32)
        egrad[i] = total.astype(BF)
        for step in (4, 2, 6, 3, 5, 1, 7):
            peer, device = g_peer(step)
            send(
                egrad.at[i, rows_of(peer)], recv_b2.at[i, rows_of(g)],
                s_b2.at[i], r_b2.at[i], device,
            )
        recv_b2[i, rows_of(g), :] = egrad[i, rows_of(g), :]

    def back_to_z(i):
        wait_all(recv_b2.at[i, pl.ds(0, MOST)], r_b2.at[i])
        out_a2[i] = nn(perm[...], recv_b2[i]).astype(BF)
        for step in (4, 3, 5, 2, 6, 1, 7):
            peer, device = z_peer(step)
            send(
                out_a2.at[i, rows_of(peer)], coming.at[i, rows_of(z)],
                s_a2.at[i], r_a2.at[i], device,
            )
        coming[i, rows_of(z), :] = out_a2[i, rows_of(z), :]

    def at_tokens(i):
        wait_all(coming.at[i, pl.ds(0, MOST)], r_a2.at[i])
        c = i - (STEPS - CH)
        if c >= 0:
            summed = nn(sel_t[:, 0:PART], coming[c]) + nn(sel_t[:, PART:ROWS], coming[i])
            mix[y, :, lanes(c)] = (cot[:, lanes(c)].astype(F32) + summed).astype(BF)
            mine = mix.at[y, :, lanes(c)]
            send(mine, mine, s_m.at[0, c], r_ml.at[c], to_right)
            send(mine, mine, s_m.at[1, c], r_mr.at[c], to_left)

    def mix_passed(c):
        size = coming.at[c, pl.ds(0, TOK)]
        wait_all(size, r_ml.at[c])
        passed = mix.at[left, pl.ds(0, TOK // 2), lanes(c)]
        send(passed, passed, s_m.at[2, c], r_nl.at[c], to_right)
        wait_all(size, r_mr.at[c])
        passed = mix.at[right, pl.ds(TOK // 2, TOK // 2), lanes(c)]
        send(passed, passed, s_m.at[3, c], r_nr.at[c], to_left)

    def mix_whole(c):
        size = coming.at[c, pl.ds(0, TOK // 2)]
        wait_all(size, r_nl.at[c])
        wait_all(size, r_nr.at[c])
        arrived = jnp.concatenate([mix[q, :, lanes(c)] for q in range(NY)], axis=1)
        proj = jnp.concatenate(
            [wp[:, pl.ds(q * WIDE + c * LANES, LANES)] for q in range(NY)], axis=1
        )
        term = nt(arrived, proj)
        dac[...] = term if c == 0 else dac[...] + term
        if c == CH - 1:
            norm_grad_sums()
        product = tn(act_c[...], arrived)
        for core_at in range(2):
            for x_at in range(NX):
                gpb[c, core_at, x_at] = jnp.concatenate(
                    [
                        product[(z_at * NG + x_at * 2 + core_at) * 8 :][:8]
                        for z_at in range(NZ)
                    ],
                    axis=0,
                ).astype(BF)
        send(gpb.at[c, 1 - core], rc.at[c], s_c.at[c], r_c.at[c], to_core)

    def core_sums(c):
        wait_all(rc.at[c], r_c.at[c])
        gx[c] = (gpb[c, core].astype(F32) + rc[c].astype(F32)).astype(BF)
        top, bottom = pl.ds(0, XROWS // 2), pl.ds(XROWS // 2, XROWS // 2)
        send(gx.at[c, x_across, top], x1l.at[c], s_x.at[0, c], r_x1l.at[c], to_x_right)
        send(gx.at[c, x_across, bottom], x1r.at[c], s_x.at[1, c], r_x1r.at[c], to_x_left)
        send(gx.at[c, x_right, bottom], xfl.at[c, bottom], s_x.at[2, c], r_xl.at[c], to_x_right)
        send(gx.at[c, x_left, top], xfr.at[c, top], s_x.at[3, c], r_xr.at[c], to_x_left)

    def x_partial(c):
        top, bottom = pl.ds(0, XROWS // 2), pl.ds(XROWS // 2, XROWS // 2)
        wait_all(x1l.at[c], r_x1l.at[c])
        xar[c] = (gx[c, x_right, top, :].astype(F32) + x1l[c].astype(F32)).astype(BF)
        send(xar.at[c], xfl.at[c, top], s_x.at[4, c], r_xl.at[c], to_x_right)
        wait_all(x1r.at[c], r_x1r.at[c])
        xal[c] = (gx[c, x_left, bottom, :].astype(F32) + x1r[c].astype(F32)).astype(BF)
        send(xal.at[c], xfr.at[c, bottom], s_x.at[5, c], r_xr.at[c], to_x_left)
        if c == CH - 2:
            conv_grad()

    def x_whole(c):
        wait_all(xfl.at[c], r_xl.at[c])
        wait_all(xfr.at[c], r_xr.at[c])
        total = gx[c, x].astype(F32) + xfl[c].astype(F32) + xfr[c].astype(F32)
        gz[c] = jnp.concatenate(
            [
                total[z_at * 8 : z_at * 8 + 8, half * 256 : half * 256 + 256]
                for z_at in range(NZ)
                for half in (0, 1)
            ],
            axis=0,
        ).astype(BF)
        for step in (4, 3, 5, 2, 6, 1, 7):
            peer, device = z_peer(step)
            send(
                gz.at[c, pl.ds(pl.multiple_of(peer * 16, 16), 16)],
                rz.at[c, pl.ds(pl.multiple_of(z * 16, 16), 16)],
                s_z.at[c], r_z.at[c], device,
            )
        own = pl.ds(pl.multiple_of(z * 16, 16), 16)
        rz[c, own, :] = gz[c, own, :]
        if c == CH - 2:
            conv_first()
        if c == CH - 1:
            conv_rest()

    def weight_grads(j):
        if j < 4:
            gd_out[:, pl.ds(j * WIDE, WIDE)] = tn(act_s[...], cotf[j]).astype(BF)
        else:
            part = pl.ds((j - 4) * 256, 256)
            both = tn(rows_p[:, part], dgu[...]).astype(BF)
            gg_out[part, :] = both[:, 0:HID]
            gu_out[part, :] = both[:, HID : 2 * HID]

    stores = [
        pltpu.make_async_copy(src, dst, s_out.at[i])
        for i, (src, dst) in enumerate(((gg_out, gg_hbm), (gu_out, gu_hbm), (gd_out, gd_hbm)))
    ]

    def norm_grad_sums():
        grad = dac[...] * fac[...]
        dac[...] = grad
        sums = [jnp.sum(v, axis=1, keepdims=True) for v in (grad, grad * xhat[...])]
        nstat[y] = columns(sums, TOK).T[0:8, :]
        for i, device in enumerate((to_right, to_left, to_across)):
            send(nstat.at[y], nstat.at[y], s_n.at[i], r_n.at[0], device)

    def conv_grad():
        wait_all(nstat.at[pl.ds(0, NY - 1)], r_n.at[0])
        total = as_columns(nstat[0] + nstat[1] + nstat[2] + nstat[3]) / CHANNELS
        ext[0:TOK, :] = rstd_s[...] * (dac[...] - total[:, 0:1] - xhat[...] * total[:, 1:2])
        send(ext.at[pl.ds(0, 32)], halo, s_h.at[0], r_h.at[0], to_before)

    def conv_rows(begin):
        part = pl.ds(begin, TOK // 2)

        def column(j, carry):
            cols = pl.ds(pl.multiple_of(j * LANES, LANES), LANES)
            total = jnp.zeros((TOK // 2, LANES), F32)
            for k in range(TAPS):
                total = total + taps[k : k + 1, cols] * ext[pl.ds(begin + TAPS - 1 - k, TOK // 2), cols]
            gv_out[part, cols] = (total * sg[part, cols]).astype(BF)
            gt_out[part, cols] = (total * vg[part, cols]).astype(BF)
            return carry

        lax.fori_loop(0, CH, column, 0)

    def conv_first():
        conv_rows(0)

    def conv_rest():
        wait_all(halo, r_h.at[0])
        keep = jnp.where(place == NZ * NG - 1, 0.0, 1.0)
        ext[TOK:EXT, :] = halo[...] * keep
        conv_rows(TOK // 2)

    stages = dict(
        Z=from_z, G=from_g, Y=from_y, D=gathered, I=input_grads, P=partial_sums, W=whole_sums,
        B=back_to_z, T=at_tokens, M=mix_passed, X=mix_whole, C=core_sums, K=x_partial, L=x_whole,
    )

    def run(order, beside):
        for name in order:
            stages[name[0]](int(name[1]))
            if beside:
                beside.pop(0)()

    run(DISPATCH, fill)
    run(BETWEEN, fill)
    grads = [functools.partial(weight_grads, j) for j in range(4)] + [stores[2].start]
    grads += [functools.partial(weight_grads, j) for j in range(4, 12)]
    grads += [stores[0].start, stores[1].start]
    run(RETURN, grads)

    for c in range(CH):
        wait_all(rz.at[c, pl.ds(0, 112)], r_z.at[c])
        total = rz[c, 0:16, :].astype(F32)
        for z_at in range(1, NZ):
            total = total + rz[c, z_at * 16 : z_at * 16 + 16, :].astype(F32)
        for q in range(NY):
            row_at, lane_at = (q // 2) * 8, (q % 2) * LANES
            gp_out[:, pl.ds(q * WIDE + c * LANES, LANES)] = total[
                row_at : row_at + 8, lane_at : lane_at + LANES
            ]

    for i in range(STEPS):
        full, most, half = out_b.at[i], out_b.at[i, pl.ds(0, MOST)], out_b.at[i, low]
        for sem in (s_a, s_b, s_b2, s_a2):
            wait_all(most, sem.at[i])
        for j, size in enumerate((full, full, half, half)):
            wait_all(size, s_y.at[j, i])
        for j in range(6):
            wait_all(half, s_rs.at[j, i])
    for c in range(CH):
        for i in range(4):
            wait_all(out_b.at[c, pl.ds(0, TOK if i < 2 else TOK // 2)], s_m.at[i, c])
        wait_all(rc.at[c], s_c.at[c])
        for i in range(6):
            wait_all(x1l.at[c], s_x.at[i, c])
        wait_all(rz.at[c, pl.ds(0, 112)], s_z.at[c])
    for i in range(3):
        wait_all(stat.at[0], s_stat.at[i])
        wait_all(nstat.at[0], s_n.at[i])
        stores[i].wait()
    wait_all(halo, s_h.at[0])


def hand_on_kernel(*refs):
    count = (len(refs) - 2) // 3
    sources, results, held = refs[:count], refs[count : 2 * count], refs[2 * count : 3 * count]
    s_in, s_out = refs[3 * count :]
    reads = [pltpu.make_async_copy(a, b, s_in.at[i]) for i, (a, b) in enumerate(zip(sources, held))]
    writes = [pltpu.make_async_copy(a, b, s_out.at[i]) for i, (a, b) in enumerate(zip(held, results))]
    for read in reads:
        read.start()
    for read, write in zip(reads, writes):
        read.wait()
        write.start()
    for write in writes:
        write.wait()


def handed_on(*arrays):
    anywhere = pl.BlockSpec(memory_space=pl.ANY)
    return pl.pallas_call(
        hand_on_kernel,
        out_shape=tuple(jax.ShapeDtypeStruct(a.shape, a.dtype) for a in arrays),
        in_specs=[anywhere] * len(arrays),
        out_specs=(anywhere,) * len(arrays),
        scratch_shapes=[pltpu.VMEM(a.shape, a.dtype) for a in arrays]
        + [pltpu.SemaphoreType.DMA((len(arrays),))] * 2,
        name="handed_on",
    )(*arrays)


def per_device(
    cot_out,
    route_ids,
    route_weight,
    expert_inputs,
    w_gate,
    w_up,
    w_down,
    w_proj,
    conv_out,
    channel_norm_gain,
    taps,
    value_pre,
    gate_pre,
):
    vmem = pl.BlockSpec(memory_space=pltpu.VMEM)
    anywhere = pl.BlockSpec(memory_space=pl.ANY)
    dma, V = pltpu.SemaphoreType.DMA, pltpu.VMEM
    chunked = V((STEPS, PART, LANES), BF)
    halves = V((STEPS, HALF, LANES), BF)
    tokens = V((TOK, WIDE), F32)
    x_half = V((CH, XROWS // 2, WIDE), BF)
    per_chunk, per_step = dma((CH,)), dma((STEPS,))
    gate_grad, up_grad, down_grad, proj_grad, grad_value, grad_gate = pl.pallas_call(
        step_kernel,
        out_shape=(
            jax.ShapeDtypeStruct((CHANNELS, HID), BF),
            jax.ShapeDtypeStruct((CHANNELS, HID), BF),
            jax.ShapeDtypeStruct((HID, CHANNELS), BF),
            jax.ShapeDtypeStruct((8, CHANNELS), F32),
            jax.ShapeDtypeStruct((TOK, WIDE), BF),
            jax.ShapeDtypeStruct((TOK, WIDE), BF),
        ),
        in_specs=[vmem] * 6 + [anywhere] * 7,
        out_specs=(anywhere,) * 3 + (vmem,) * 3,
        scratch_shapes=[
            V((ROWS, CHANNELS), BF), V((CHANNELS, HID), BF), V((CHANNELS, HID), BF),
            V((HID, CHANNELS), BF), V((WIDE, CHANNELS), BF), V((TOK, WIDE), BF), V((TOK, WIDE), BF),
            V((CHANNELS, HID), BF), V((CHANNELS, HID), BF), V((HID, CHANNELS), BF),
            V((PART, PART), BF), V((PART, ROWS), BF),
            chunked, chunked, chunked,
            V((NY, ROWS, WIDE), BF),
            V((ROWS, HID), BF), V((ROWS, HID), F32), V((ROWS, HID), F32), V((ROWS, HID), F32),
            V((ROWS, HID), F32),
            V((ROWS, 2 * HID), BF), V((TOK, ROWS), BF), V((ROWS, CHANNELS), BF),
            V((STEPS, NY, PART, LANES), BF),
            halves, halves, halves, halves,
            chunked, chunked, chunked, chunked, chunked, chunked,
            V((NY, TOK, WIDE), BF),
            V((NY, 8, TOK), F32), V((NY, 8, TOK), F32),
            tokens, V((TOK, WIDE), BF), tokens, V((TOK, 1), F32), tokens, tokens, tokens,
            V((EXT, WIDE), F32), V((32, WIDE), F32),
            V((CH, 2, NX, XROWS, WIDE), BF), V((CH, NX, XROWS, WIDE), BF),
            V((CH, NX, XROWS, WIDE), BF),
            x_half, x_half, x_half, x_half,
            V((CH, XROWS, WIDE), BF), V((CH, XROWS, WIDE), BF),
            V((CH, 2 * XROWS, WIDE // 2), BF), V((CH, 2 * XROWS, WIDE // 2), BF),
            dma((7,)), dma((3,)),
            per_step, per_step, per_step, per_step,
            dma((4, STEPS)), per_step, per_step, per_step, per_step,
            dma((6, STEPS)), per_step, per_step, per_step, per_step,
            per_step, per_step, per_step, per_step,
            dma((4, CH)), per_chunk, per_chunk, per_chunk, per_chunk,
            dma((3,)), dma((1,)), dma((3,)), dma((1,)), dma((1,)), dma((1,)),
            per_chunk, per_chunk, dma((6, CH)), per_chunk, per_chunk, per_chunk, per_chunk,
            per_chunk, per_chunk,
        ],
        compiler_params=pltpu.CompilerParams(
            collective_id=0, has_side_effects=True, vmem_limit_bytes=62 * 1024 * 1024
        ),
        name="step",
    )(
        cot_out, route_ids.T, route_weight.T, conv_out, channel_norm_gain[None, :], taps,
        expert_inputs[0], w_gate[0], w_up[0], w_down[0], w_proj, value_pre, gate_pre,
    )
    gate_grad, up_grad, down_grad, proj_grad, grad_value, grad_gate = handed_on(
        gate_grad, up_grad, down_grad, proj_grad, grad_value, grad_gate
    )
    return gate_grad[None], up_grad[None], down_grad[None], proj_grad, grad_value, grad_gate


def solution(mesh):
    finer = Mesh(mesh.devices.reshape(8, 4, 2, mesh.shape["tp"]), ("sp_0", "sp_1", "sp_2", "tp"))
    placed = (
        P(SP, "tp"),
        P(SP, None),
        P(SP, None),
        P(SP, None, None),
        P(SP, None, "tp"),
        P(SP, None, "tp"),
        P(SP, "tp", None),
        P("tp", None),
        P(SP, "tp"),
        P("tp"),
        P(None, "tp"),
        P(SP, "tp"),
        P(SP, "tp"),
    )
    return jax.shard_map(
        per_device,
        mesh=finer,
        in_specs=placed,
        out_specs=(
            P(SP, None, "tp"),
            P(SP, None, "tp"),
            P(SP, "tp", None),
            P(TP_SP, None),
            P(SP, "tp"),
            P(SP, "tp"),
        ),
        check_vma=False,
    )
```

```python
import functools

import jax
import jax.numpy as jnp
from jax import lax
from jax.experimental import pallas as pl
from jax.experimental.pallas import tpu as pltpu
from jax.sharding import Mesh
from jax.sharding import PartitionSpec as P

SP = ("sp_0", "sp_1", "sp_2")
TP_SP = ("tp", "sp_0", "sp_1", "sp_2")
MESH = pl.DeviceIdType.MESH

clamp_limit = 7.0
swish_alpha = 1.702
norm_epsilon = 1e-05

CH = 4
LANES = 128
NZ = 8
NG = 8
NY = 4
CAP = 12
HALVES = 2
SUB = CAP // HALVES
STEPS = HALVES * CH
BLOCK = NZ * SUB
PART = NZ * BLOCK
ROWS = HALVES * PART
HALF = PART // 2
MOST = PART - BLOCK
TOK = 256
WIDE = CH * LANES
HID = 256
TAPS = 31
FIRST_FILL = 8
AHEAD = 2
DISPATCH = (
    "Z0", "Z1", "G0", "Z2", "G1", "Z3", "G2", "Y0", "Z4", "G3", "Y1", "D0", "Z5", "G4", "Y2",
    "D1", "Z6", "G5", "Y3", "D2", "Z7", "G6", "Y4", "G7", "D3", "I0",
)
BETWEEN = (
    "Y5", "D4", "P0", "Y6", "D5", "P1", "Y7", "D6", "P2", "D7", "I1",
)
RETURN = (
    "P3", "W0", "W1", "P4", "W2", "W3", "B0", "B1", "P5", "B2", "W4", "B3", "P6", "W5",
    "T0", "B4", "T1", "P7", "W6", "T2", "B5", "T3", "W7", "B6", "T4", "B7", "T5", "M0",
    "T6", "M1", "X0", "T7", "M2", "X1", "C0", "M3", "X2", "C1", "X3", "K0", "C2", "K1",
    "L0", "C3", "K2", "L1", "K3", "L2", "L3",
)
EXT = TOK + 32
CHANNELS = 2048
NX = 4
XROWS = 64
BF = jnp.bfloat16
F32 = jnp.float32


def nt(a, b):
    return lax.dot_general(a, b, (((1,), (1,)), ((), ())), preferred_element_type=F32)


def tn(a, b):
    return lax.dot_general(a, b, (((0,), (0,)), ((), ())), preferred_element_type=F32)


def nn(a, b):
    return lax.dot_general(a, b, (((1,), (0,)), ((), ())), preferred_element_type=F32)


def wait_all(ref, sem):
    pltpu.make_async_copy(ref, ref, sem).wait()


def send(src, dst, send_sem, recv_sem, device):
    pltpu.make_async_remote_copy(
        src_ref=src,
        dst_ref=dst,
        send_sem=send_sem,
        recv_sem=recv_sem,
        device_id=device,
        device_id_type=MESH,
    ).start()


def lanes(c):
    return pl.ds(c * LANES, LANES)


def rows_of(block):
    return pl.ds(pl.multiple_of(block * BLOCK, BLOCK), BLOCK)


def columns(parts, rows):
    lane = lax.broadcasted_iota(jnp.int32, (rows, LANES), 1)
    whole = jnp.zeros((rows, LANES), F32)
    for i, part in enumerate(parts):
        whole = jnp.where(lane == i, part, whole)
    return whole


def as_columns(rows8):
    return jnp.concatenate([rows8, jnp.zeros((LANES - 8, TOK), F32)], axis=0).T


def digits(at, low, high):
    rest = jnp.floor((at + 0.5) * (1.0 / low))
    top = jnp.floor((rest + 0.5) * (1.0 / high))
    return top, rest - high * top, at - low * rest


def hot_rows(source, count):
    lane = lax.broadcasted_iota(jnp.int32, (source.shape[0], count), 1).astype(F32)
    return jnp.where(lane == source, 1.0, 0.0).astype(BF)


def swap_matrix():
    at = lax.broadcasted_iota(jnp.int32, (PART, 1), 0).astype(F32)
    b, a, slot = digits(at, SUB, NZ)
    return hot_rows(a * BLOCK + b * SUB + slot, PART)


def order_matrix(half):
    at = lax.broadcasted_iota(jnp.int32, (PART, 1), 0).astype(F32)
    g, z, slot = digits(at, SUB, NZ)
    return hot_rows((z * NG + g) * CAP + half * SUB + slot, ROWS)


def step_kernel(
    cot, ids, route_w, conv, gain, taps, rows_hbm, wg_hbm, wu_hbm, wd_hbm, wp_hbm, value_hbm, gate_hbm,
    gg_hbm, gu_hbm, gd_hbm, gp_out, gv_out, gt_out,
    rows_in, wg, wu, wd, wp, value, gate, gg_out, gu_out, gd_out,
    perm, order, out_a, recv_a, out_b, cotf, act_s, f_up, f_gate, dact, up_rest, dgu, sel_t, rows_p,
    partial, r1l, r1r, accl, accr, from_l, from_r, egrad, recv_b2, out_a2, coming, mix,
    stat, nstat, xhat, act_c, fac, rstd_s, sg, vg, dac, ext, halo,
    gpb, rc, gx, x1l, x1r, xal, xar, xfl, xfr, gz, rz,
    s_in, s_out,
    s_a, r_a, s_b, r_b, s_y, r_yl, r_yr, r_fl, r_fr,
    s_rs, r_1l, r_1r, r_sl, r_sr, s_b2, r_b2, s_a2, r_a2, s_m, r_ml, r_mr, r_nl, r_nr,
    s_stat, r_stat, s_n, r_n, s_h, r_h,
    s_c, r_c, s_x, r_x1l, r_x1r, r_xl, r_xr, s_z, r_z,
):
    z = lax.axis_index("sp_0")
    x = lax.axis_index("sp_1")
    core = lax.axis_index("sp_2")
    g = x * 2 + core
    y = lax.axis_index("tp")
    right, left, across = lax.rem(y + 1, NY), lax.rem(y + 3, NY), lax.rem(y + 2, NY)
    to_right, to_left, to_across = {"tp": right}, {"tp": left}, {"tp": across}
    x_right, x_left, x_across = lax.rem(x + 1, NX), lax.rem(x + 3, NX), lax.rem(x + 2, NX)
    to_x_right, to_x_left = {"sp_1": x_right}, {"sp_1": x_left}
    to_core = {"sp_2": 1 - core}
    place = z * NG + g

    def z_peer(step):
        peer = lax.rem(z + step, NZ)
        return peer, {"sp_0": peer}

    def g_peer(step):
        peer = lax.rem(g + step, NG)
        return peer, {"sp_1": peer // 2, "sp_2": lax.rem(peer, 2)}

    def in_line(step):
        other = lax.rem(place + step, NZ * NG)
        return {"sp_0": other // NG, "sp_1": lax.rem(other // 2, NX), "sp_2": lax.rem(other, 2)}

    to_before = in_line(NZ * NG - 1)
    barrier = pltpu.get_barrier_semaphore()
    greeted = [z_peer(step)[1] for step in range(1, NZ)] + [g_peer(step)[1] for step in range(1, NG)]
    greeted += [to_right, to_left, to_across, to_before, in_line(1)]
    for device in greeted:
        pl.semaphore_signal(barrier, inc=1, device_id=device, device_id_type=MESH)

    fetches = [
        pltpu.make_async_copy(src, dst, s_in.at[i])
        for i, (src, dst) in enumerate(
            ((rows_hbm, rows_in), (wg_hbm, wg), (wu_hbm, wu), (wd_hbm, wd),
             (gate_hbm, gate), (value_hbm, value), (wp_hbm, wp))
        )
    ]
    for fetch in fetches:
        fetch.start()

    t_sub = lax.broadcasted_iota(jnp.int32, (TOK, TOK), 0)
    t_lane = lax.broadcasted_iota(jnp.int32, (TOK, TOK), 1)
    before, after = t_sub < t_lane, t_lane < t_sub
    row = [ids[k : k + 1, :].astype(F32) for k in (0, 1)]
    w_r = [route_w[k : k + 1, :] for k in (0, 1)]
    turned = as_columns(jnp.concatenate(row + [jnp.zeros((6, TOK), F32)], axis=0))
    col = [turned[:, k : k + 1] for k in (0, 1)]

    def row_of(slot, expert):
        return slot + SUB * expert + jnp.where(slot >= SUB, 1.0 * (PART - SUB), 0.0)

    slot_r = lax.broadcasted_iota(jnp.int32, (ROWS, TOK), 0).astype(F32)
    chosen, weight = None, None
    for k in (0, 1):
        same = ((col[0] == row[k]) | (col[1] == row[k])) & before
        dest = row_of(jnp.sum(jnp.where(same, 1.0, 0.0), axis=0, keepdims=True), row[k])
        hot = slot_r == dest
        one, scale = jnp.where(hot, 1.0, 0.0), jnp.where(hot, w_r[k], 0.0)
        chosen = one if chosen is None else chosen + one
        weight = scale if weight is None else weight + scale
    chosen = chosen.astype(BF)
    weight = jnp.sum(weight, axis=1, keepdims=True)

    for i in range(STEPS):
        c, part = i % CH, slice(i // CH * PART, i // CH * PART + PART)
        out_a[i] = (weight[part] * nn(chosen[part], cot[:, lanes(c)])).astype(BF)
        if i == 0:
            pl.semaphore_wait(barrier, len(greeted))
        for step in (4, 3, 5, 2, 6, 1, 7):
            peer, device = z_peer(step)
            send(out_a.at[i, rows_of(peer)], recv_a.at[i, rows_of(z)], s_a.at[i], r_a.at[i], device)
        recv_a[i, rows_of(z), :] = out_a[i, rows_of(z), :]

    wide = conv[...].astype(F32)
    sums = [jnp.sum(v, axis=1, keepdims=True) for v in (wide, wide * wide)]
    stat[y] = columns(sums, TOK).T[0:8, :]
    for i, device in enumerate((to_right, to_left, to_across)):
        send(stat.at[y], stat.at[y], s_stat.at[i], r_stat.at[0], device)

    perm[...] = swap_matrix()

    def unpack_slots():
        slot_c = lax.broadcasted_iota(jnp.int32, (TOK, ROWS), 1).astype(F32)
        back = None
        for k in (0, 1):
            same = ((row[0] == col[k]) | (row[1] == col[k])) & after
            dest = row_of(jnp.sum(jnp.where(same, 1.0, 0.0), axis=1, keepdims=True), col[k])
            one = jnp.where(slot_c == dest, 1.0, 0.0)
            back = one if back is None else back + one
        sel_t[...] = back.astype(BF)

    def forward_rows(half, j):
        if j == 0:
            if half == 0:
                fetches[0].wait()
            order[...] = order_matrix(half)
        cols = pl.ds(j * 512, 512)
        rows_p[pl.ds(half * PART, PART), cols] = nn(order[...], rows_in[:, cols]).astype(BF)

    def forward_sums(j):
        total, w = ((f_gate, wg), (f_up, wu), (dact, wg), (up_rest, wu))[j]
        if j < 2:
            fetches[j + 1].wait()
        half = pl.ds(j // 2 * (CHANNELS // 2), CHANNELS // 2)
        total[...] = nn(rows_p[:, half], w[half, :])

    def forward_part(j):
        part = pl.ds(j * 256, 256)
        gate_lin = f_gate[part, :] + dact[part, :]
        up_lin = f_up[part, :] + up_rest[part, :]
        gate_c = jnp.minimum(gate_lin, clamp_limit)
        up_c = jnp.clip(up_lin, -clamp_limit, clamp_limit)
        sig = jax.nn.sigmoid(swish_alpha * gate_c)
        act_s[part, :] = ((up_c + 1.0) * gate_c * sig).astype(BF)
        up_open = (up_lin > -clamp_limit) & (up_lin < clamp_limit)
        f_up[part, :] = jnp.where(up_open, gate_c * sig, 0.0)
        slope = (up_c + 1.0) * (sig + swish_alpha * gate_c * sig * (1.0 - sig))
        f_gate[part, :] = jnp.where(gate_lin < clamp_limit, slope, 0.0)

    def norm_terms():
        wait_all(stat.at[pl.ds(0, NY - 1)], r_stat.at[0])
        total = as_columns(stat[0] + stat[1] + stat[2] + stat[3])
        mean = total[:, 0:1] / CHANNELS
        var = total[:, 1:2] / CHANNELS - mean * mean
        rstd = lax.rsqrt(var + norm_epsilon)
        rstd_s[...] = rstd
        normalized = (conv[...].astype(F32) - mean) * rstd
        xhat[...] = normalized
        normed = normalized * gain[...]
        s = jax.nn.sigmoid(normed)
        act_c[...] = (normed * s).T.astype(BF)
        fac[...] = s * (1.0 + normed * (1.0 - s)) * gain[...]

    def glu_terms():
        fetches[4].wait()
        fetches[5].wait()
        gate_sig = jax.nn.sigmoid(gate[...].astype(F32))
        sg[...] = gate_sig
        vg[...] = value[...].astype(F32) * gate_sig * (1.0 - gate_sig)
        fetches[6].wait()

    fill = [functools.partial(forward_rows, half, j) for half in range(HALVES) for j in range(4)]
    fill += [functools.partial(forward_sums, j) for j in range(4)]
    fill += [functools.partial(forward_part, j) for j in range(3)]
    fill += [fetches[3].wait, norm_terms, unpack_slots, glu_terms]
    for _ in range(FIRST_FILL):
        fill.pop(0)()

    def rows_at(i):
        return pl.ds(i // CH * PART, PART)

    def half_at(i, which):
        return pl.ds(i // CH * PART + which * HALF, HALF)

    low, high = pl.ds(0, HALF), pl.ds(HALF, HALF)

    def from_z(i):
        wait_all(recv_a.at[i, pl.ds(0, MOST)], r_a.at[i])
        out_b[i] = nn(perm[...], recv_a[i]).astype(BF)
        mine = pl.ds(pl.multiple_of(i // CH * PART + g * BLOCK, BLOCK), BLOCK)
        for step in (4, 2, 6, 3, 5, 1, 7):
            peer, device = g_peer(step)
            send(
                out_b.at[i, rows_of(peer)], cotf.at[y, mine, lanes(i % CH)],
                s_b.at[i], r_b.at[i], device,
            )
        cotf[y, mine, lanes(i % CH)] = out_b[i, rows_of(g), :]

    def from_g(i):
        wait_all(out_b.at[i, pl.ds(0, MOST)], r_b.at[i])
        mine = cotf.at[y, rows_at(i), lanes(i % CH)]
        send(mine, mine, s_y.at[0, i], r_yl.at[i], to_right)
        send(mine, mine, s_y.at[1, i], r_yr.at[i], to_left)

    def from_y(i):
        wait_all(out_b.at[i], r_yl.at[i])
        passed = cotf.at[left, half_at(i, 0), lanes(i % CH)]
        send(passed, passed, s_y.at[2, i], r_fl.at[i], to_right)
        wait_all(out_b.at[i], r_yr.at[i])
        passed = cotf.at[right, half_at(i, 1), lanes(i % CH)]
        send(passed, passed, s_y.at[3, i], r_fr.at[i], to_left)

    def gathered(i):
        c, part = i % CH, rows_at(i)
        wait_all(out_b.at[i, low], r_fl.at[i])
        wait_all(out_b.at[i, low], r_fr.at[i])
        arrived = jnp.concatenate([cotf[q, part, lanes(c)] for q in range(NY)], axis=1)
        down = jnp.concatenate(
            [wd[:, pl.ds(q * WIDE + c * LANES, LANES)] for q in range(NY)], axis=1
        )
        term = nt(arrived, down)
        dact[part, :] = term if c == 0 else dact[part, :] + term

    def first_partials(i):
        send(partial.at[i, across, low], r1l.at[i], s_rs.at[0, i], r_1l.at[i], to_right)
        send(partial.at[i, across, high], r1r.at[i], s_rs.at[1, i], r_1r.at[i], to_left)
        send(partial.at[i, right, high], from_l.at[i, high], s_rs.at[2, i], r_sl.at[i], to_right)
        send(partial.at[i, left, low], from_r.at[i, low], s_rs.at[3, i], r_sr.at[i], to_left)

    def input_grads(half):
        part = pl.ds(half * PART, PART)
        dgu[part, 0:HID] = (dact[part, :] * f_gate[part, :]).astype(BF)
        dgu[part, HID : 2 * HID] = (dact[part, :] * f_up[part, :]).astype(BF)
        for c in range(CH):
            i = half * CH + c
            weights = jnp.concatenate(
                [
                    jnp.concatenate(
                        [w[pl.ds(q * WIDE + c * LANES, LANES), :] for w in (wg, wu)], axis=1
                    )
                    for q in range(NY)
                ],
                axis=0,
            )
            product = nt(dgu[part, :], weights).astype(BF)
            for q in range(NY):
                partial[i, q] = product[:, q * LANES : (q + 1) * LANES]
            if c < AHEAD:
                first_partials(i)

    def partial_sums(i):
        wait_all(r1l.at[i], r_1l.at[i])
        accr[i] = (partial[i, right, low, :].astype(F32) + r1l[i].astype(F32)).astype(BF)
        send(accr.at[i], from_l.at[i, low], s_rs.at[4, i], r_sl.at[i], to_right)
        wait_all(r1r.at[i], r_1r.at[i])
        accl[i] = (partial[i, left, high, :].astype(F32) + r1r[i].astype(F32)).astype(BF)
        send(accl.at[i], from_r.at[i, high], s_rs.at[5, i], r_sr.at[i], to_left)
        if i % CH + AHEAD < CH:
            first_partials(i + AHEAD)

    def whole_sums(i):
        wait_all(from_l.at[i], r_sl.at[i])
        wait_all(from_r.at[i], r_sr.at[i])
        total = partial[i, y].astype(F32) + from_l[i].astype(F32) + from_r[i].astype(F32)
        egrad[i] = total.astype(BF)
        for step in (4, 2, 6, 3, 5, 1, 7):
            peer, device = g_peer(step)
            send(
                egrad.at[i, rows_of(peer)], recv_b2.at[i, rows_of(g)],
                s_b2.at[i], r_b2.at[i], device,
            )
        recv_b2[i, rows_of(g), :] = egrad[i, rows_of(g), :]

    def back_to_z(i):
        wait_all(recv_b2.at[i, pl.ds(0, MOST)], r_b2.at[i])
        out_a2[i] = nn(perm[...], recv_b2[i]).astype(BF)
        for step in (4, 3, 5, 2, 6, 1, 7):
            peer, device = z_peer(step)
            send(
                out_a2.at[i, rows_of(peer)], coming.at[i, rows_of(z)],
                s_a2.at[i], r_a2.at[i], device,
            )
        coming[i, rows_of(z), :] = out_a2[i, rows_of(z), :]

    def at_tokens(i):
        wait_all(coming.at[i, pl.ds(0, MOST)], r_a2.at[i])
        c = i - (STEPS - CH)
        if c < 0:
            first = nn(sel_t[:, 0:PART], coming[i])
            ext[0:TOK, lanes(i)] = cot[:, lanes(i)].astype(F32) + first
        else:
            summed = ext[0:TOK, lanes(c)] + nn(sel_t[:, PART:ROWS], coming[i])
            mix[y, :, lanes(c)] = summed.astype(BF)
            mine = mix.at[y, :, lanes(c)]
            send(mine, mine, s_m.at[0, c], r_ml.at[c], to_right)
            send(mine, mine, s_m.at[1, c], r_mr.at[c], to_left)

    def mix_passed(c):
        size = coming.at[c, pl.ds(0, TOK)]
        wait_all(size, r_ml.at[c])
        passed = mix.at[left, pl.ds(0, TOK // 2), lanes(c)]
        send(passed, passed, s_m.at[2, c], r_nl.at[c], to_right)
        wait_all(size, r_mr.at[c])
        passed = mix.at[right, pl.ds(TOK // 2, TOK // 2), lanes(c)]
        send(passed, passed, s_m.at[3, c], r_nr.at[c], to_left)

    def mix_whole(c):
        size = coming.at[c, pl.ds(0, TOK // 2)]
        wait_all(size, r_nl.at[c])
        wait_all(size, r_nr.at[c])
        arrived = jnp.concatenate([mix[q, :, lanes(c)] for q in range(NY)], axis=1)
        proj = jnp.concatenate(
            [wp[:, pl.ds(q * WIDE + c * LANES, LANES)] for q in range(NY)], axis=1
        )
        term = nt(arrived, proj)
        dac[...] = term if c == 0 else dac[...] + term
        if c == CH - 1:
            norm_grad_sums()
        product = nn(act_c[...], arrived)
        for core_at in range(2):
            for x_at in range(NX):
                gpb[c, core_at, x_at] = jnp.concatenate(
                    [
                        product[(z_at * NG + x_at * 2 + core_at) * 8 :][:8]
                        for z_at in range(NZ)
                    ],
                    axis=0,
                ).astype(BF)
        send(gpb.at[c, 1 - core], rc.at[c], s_c.at[c], r_c.at[c], to_core)

    def core_sums(c):
        wait_all(rc.at[c], r_c.at[c])
        gx[c] = (gpb[c, core].astype(F32) + rc[c].astype(F32)).astype(BF)
        top, bottom = pl.ds(0, XROWS // 2), pl.ds(XROWS // 2, XROWS // 2)
        send(gx.at[c, x_across, top], x1l.at[c], s_x.at[0, c], r_x1l.at[c], to_x_right)
        send(gx.at[c, x_across, bottom], x1r.at[c], s_x.at[1, c], r_x1r.at[c], to_x_left)
        send(gx.at[c, x_right, bottom], xfl.at[c, bottom], s_x.at[2, c], r_xl.at[c], to_x_right)
        send(gx.at[c, x_left, top], xfr.at[c, top], s_x.at[3, c], r_xr.at[c], to_x_left)

    def x_partial(c):
        top, bottom = pl.ds(0, XROWS // 2), pl.ds(XROWS // 2, XROWS // 2)
        wait_all(x1l.at[c], r_x1l.at[c])
        xar[c] = (gx[c, x_right, top, :].astype(F32) + x1l[c].astype(F32)).astype(BF)
        send(xar.at[c], xfl.at[c, top], s_x.at[4, c], r_xl.at[c], to_x_right)
        wait_all(x1r.at[c], r_x1r.at[c])
        xal[c] = (gx[c, x_left, bottom, :].astype(F32) + x1r[c].astype(F32)).astype(BF)
        send(xal.at[c], xfr.at[c, bottom], s_x.at[5, c], r_xr.at[c], to_x_left)
        if c == CH - 2:
            conv_grad()

    def x_whole(c):
        wait_all(xfl.at[c], r_xl.at[c])
        wait_all(xfr.at[c], r_xr.at[c])
        total = gx[c, x].astype(F32) + xfl[c].astype(F32) + xfr[c].astype(F32)
        gz[c] = jnp.concatenate(
            [
                total[z_at * 8 : z_at * 8 + 8, half * 256 : half * 256 + 256]
                for z_at in range(NZ)
                for half in (0, 1)
            ],
            axis=0,
        ).astype(BF)
        for step in (4, 3, 5, 2, 6, 1, 7):
            peer, device = z_peer(step)
            send(
                gz.at[c, pl.ds(pl.multiple_of(peer * 16, 16), 16)],
                rz.at[c, pl.ds(pl.multiple_of(z * 16, 16), 16)],
                s_z.at[c], r_z.at[c], device,
            )
        own = pl.ds(pl.multiple_of(z * 16, 16), 16)
        rz[c, own, :] = gz[c, own, :]
        if c == CH - 2:
            conv_first()
        if c == CH - 1:
            conv_rest()

    def weight_grads(j):
        if j < 4:
            gd_out[:, pl.ds(j * WIDE, WIDE)] = tn(act_s[...], cotf[j]).astype(BF)
        else:
            part = pl.ds((j - 4) * 256, 256)
            both = tn(rows_p[:, part], dgu[...]).astype(BF)
            gg_out[part, :] = both[:, 0:HID]
            gu_out[part, :] = both[:, HID : 2 * HID]

    stores = [
        pltpu.make_async_copy(src, dst, s_out.at[i])
        for i, (src, dst) in enumerate(((gg_out, gg_hbm), (gu_out, gu_hbm), (gd_out, gd_hbm)))
    ]

    def norm_grad_sums():
        grad = dac[...] * fac[...]
        dac[...] = grad
        sums = [jnp.sum(v, axis=1, keepdims=True) for v in (grad, grad * xhat[...])]
        nstat[y] = columns(sums, TOK).T[0:8, :]
        for i, device in enumerate((to_right, to_left, to_across)):
            send(nstat.at[y], nstat.at[y], s_n.at[i], r_n.at[0], device)

    def conv_grad():
        wait_all(nstat.at[pl.ds(0, NY - 1)], r_n.at[0])
        total = as_columns(nstat[0] + nstat[1] + nstat[2] + nstat[3]) / CHANNELS
        ext[0:TOK, :] = rstd_s[...] * (dac[...] - total[:, 0:1] - xhat[...] * total[:, 1:2])
        send(ext.at[pl.ds(0, 32)], halo, s_h.at[0], r_h.at[0], to_before)

    def conv_rows(begin):
        part = pl.ds(begin, TOK // 2)

        def column(j, carry):
            cols = pl.ds(pl.multiple_of(j * LANES, LANES), LANES)
            total = jnp.zeros((TOK // 2, LANES), F32)
            for k in range(TAPS):
                total = total + taps[k : k + 1, cols] * ext[pl.ds(begin + TAPS - 1 - k, TOK // 2), cols]
            gv_out[part, cols] = (total * sg[part, cols]).astype(BF)
            gt_out[part, cols] = (total * vg[part, cols]).astype(BF)
            return carry

        lax.fori_loop(0, CH, column, 0)

    def conv_first():
        conv_rows(0)

    def conv_rest():
        wait_all(halo, r_h.at[0])
        keep = jnp.where(place == NZ * NG - 1, 0.0, 1.0)
        ext[TOK:EXT, :] = halo[...] * keep
        conv_rows(TOK // 2)

    stages = dict(
        Z=from_z, G=from_g, Y=from_y, D=gathered, I=input_grads, P=partial_sums, W=whole_sums,
        B=back_to_z, T=at_tokens, M=mix_passed, X=mix_whole, C=core_sums, K=x_partial, L=x_whole,
    )

    def run(order, beside):
        for name in order:
            stages[name[0]](int(name[1]))
            if beside:
                beside.pop(0)()

    run(DISPATCH, fill)
    run(BETWEEN, fill)
    grads = [functools.partial(weight_grads, j) for j in range(4)] + [stores[2].start]
    grads += [functools.partial(weight_grads, j) for j in range(4, 12)]
    grads += [stores[0].start, stores[1].start]
    run(RETURN, grads)

    for c in range(CH):
        wait_all(rz.at[c, pl.ds(0, 112)], r_z.at[c])
        total = rz[c, 0:16, :].astype(F32)
        for z_at in range(1, NZ):
            total = total + rz[c, z_at * 16 : z_at * 16 + 16, :].astype(F32)
        for q in range(NY):
            row_at, lane_at = (q // 2) * 8, (q % 2) * LANES
            gp_out[:, pl.ds(q * WIDE + c * LANES, LANES)] = total[
                row_at : row_at + 8, lane_at : lane_at + LANES
            ]

    for i in range(STEPS):
        full, most, half = out_b.at[i], out_b.at[i, pl.ds(0, MOST)], out_b.at[i, low]
        for sem in (s_a, s_b, s_b2, s_a2):
            wait_all(most, sem.at[i])
        for j, size in enumerate((full, full, half, half)):
            wait_all(size, s_y.at[j, i])
        for j in range(6):
            wait_all(half, s_rs.at[j, i])
    for c in range(CH):
        for i in range(4):
            wait_all(out_b.at[c, pl.ds(0, TOK if i < 2 else TOK // 2)], s_m.at[i, c])
        wait_all(rc.at[c], s_c.at[c])
        for i in range(6):
            wait_all(x1l.at[c], s_x.at[i, c])
        wait_all(rz.at[c, pl.ds(0, 112)], s_z.at[c])
    for i in range(3):
        wait_all(stat.at[0], s_stat.at[i])
        wait_all(nstat.at[0], s_n.at[i])
        stores[i].wait()
    wait_all(halo, s_h.at[0])


def hand_on_kernel(*refs):
    count = (len(refs) - 2) // 3
    sources, results, held = refs[:count], refs[count : 2 * count], refs[2 * count : 3 * count]
    s_in, s_out = refs[3 * count :]
    reads = [pltpu.make_async_copy(a, b, s_in.at[i]) for i, (a, b) in enumerate(zip(sources, held))]
    writes = [pltpu.make_async_copy(a, b, s_out.at[i]) for i, (a, b) in enumerate(zip(held, results))]
    for read in reads:
        read.start()
    for read, write in zip(reads, writes):
        read.wait()
        write.start()
    for write in writes:
        write.wait()


def handed_on(*arrays):
    anywhere = pl.BlockSpec(memory_space=pl.ANY)
    return pl.pallas_call(
        hand_on_kernel,
        out_shape=tuple(jax.ShapeDtypeStruct(a.shape, a.dtype) for a in arrays),
        in_specs=[anywhere] * len(arrays),
        out_specs=(anywhere,) * len(arrays),
        scratch_shapes=[pltpu.VMEM(a.shape, a.dtype) for a in arrays]
        + [pltpu.SemaphoreType.DMA((len(arrays),))] * 2,
        name="handed_on",
    )(*arrays)


def per_device(
    cot_out,
    route_ids,
    route_weight,
    expert_inputs,
    w_gate,
    w_up,
    w_down,
    w_proj,
    conv_out,
    channel_norm_gain,
    taps,
    value_pre,
    gate_pre,
):
    vmem = pl.BlockSpec(memory_space=pltpu.VMEM)
    anywhere = pl.BlockSpec(memory_space=pl.ANY)
    dma, V = pltpu.SemaphoreType.DMA, pltpu.VMEM
    chunked = V((STEPS, PART, LANES), BF)
    halves = V((STEPS, HALF, LANES), BF)
    tokens = V((TOK, WIDE), F32)
    x_half = V((CH, XROWS // 2, WIDE), BF)
    per_chunk, per_step = dma((CH,)), dma((STEPS,))
    gate_grad, up_grad, down_grad, proj_grad, grad_value, grad_gate = pl.pallas_call(
        step_kernel,
        out_shape=(
            jax.ShapeDtypeStruct((CHANNELS, HID), BF),
            jax.ShapeDtypeStruct((CHANNELS, HID), BF),
            jax.ShapeDtypeStruct((HID, CHANNELS), BF),
            jax.ShapeDtypeStruct((8, CHANNELS), F32),
            jax.ShapeDtypeStruct((TOK, WIDE), BF),
            jax.ShapeDtypeStruct((TOK, WIDE), BF),
        ),
        in_specs=[vmem] * 6 + [anywhere] * 7,
        out_specs=(anywhere,) * 3 + (vmem,) * 3,
        scratch_shapes=[
            V((ROWS, CHANNELS), BF), V((CHANNELS, HID), BF), V((CHANNELS, HID), BF),
            V((HID, CHANNELS), BF), V((WIDE, CHANNELS), BF), V((TOK, WIDE), BF), V((TOK, WIDE), BF),
            V((CHANNELS, HID), BF), V((CHANNELS, HID), BF), V((HID, CHANNELS), BF),
            V((PART, PART), BF), V((PART, ROWS), BF),
            chunked, chunked, chunked,
            V((NY, ROWS, WIDE), BF),
            V((ROWS, HID), BF), V((ROWS, HID), F32), V((ROWS, HID), F32), V((ROWS, HID), F32),
            V((ROWS, HID), F32),
            V((ROWS, 2 * HID), BF), V((TOK, ROWS), BF), V((ROWS, CHANNELS), BF),
            V((STEPS, NY, PART, LANES), BF),
            halves, halves, halves, halves,
            chunked, chunked, chunked, chunked, chunked, chunked,
            V((NY, TOK, WIDE), BF),
            V((NY, 8, TOK), F32), V((NY, 8, TOK), F32),
            tokens, V((WIDE, TOK), BF), tokens, V((TOK, 1), F32), tokens, tokens, tokens,
            V((EXT, WIDE), F32), V((32, WIDE), F32),
            V((CH, 2, NX, XROWS, WIDE), BF), V((CH, NX, XROWS, WIDE), BF),
            V((CH, NX, XROWS, WIDE), BF),
            x_half, x_half, x_half, x_half,
            V((CH, XROWS, WIDE), BF), V((CH, XROWS, WIDE), BF),
            V((CH, 2 * XROWS, WIDE // 2), BF), V((CH, 2 * XROWS, WIDE // 2), BF),
            dma((7,)), dma((3,)),
            per_step, per_step, per_step, per_step,
            dma((4, STEPS)), per_step, per_step, per_step, per_step,
            dma((6, STEPS)), per_step, per_step, per_step, per_step,
            per_step, per_step, per_step, per_step,
            dma((4, CH)), per_chunk, per_chunk, per_chunk, per_chunk,
            dma((3,)), dma((1,)), dma((3,)), dma((1,)), dma((1,)), dma((1,)),
            per_chunk, per_chunk, dma((6, CH)), per_chunk, per_chunk, per_chunk, per_chunk,
            per_chunk, per_chunk,
        ],
        compiler_params=pltpu.CompilerParams(
            collective_id=0, has_side_effects=True, vmem_limit_bytes=62 * 1024 * 1024
        ),
        name="step",
    )(
        cot_out, route_ids.T, route_weight.T, conv_out, channel_norm_gain[None, :], taps,
        expert_inputs[0], w_gate[0], w_up[0], w_down[0], w_proj, value_pre, gate_pre,
    )
    gate_grad, up_grad, down_grad, proj_grad, grad_value, grad_gate = handed_on(
        gate_grad, up_grad, down_grad, proj_grad, grad_value, grad_gate
    )
    return gate_grad[None], up_grad[None], down_grad[None], proj_grad, grad_value, grad_gate


def solution(mesh):
    finer = Mesh(mesh.devices.reshape(8, 4, 2, mesh.shape["tp"]), ("sp_0", "sp_1", "sp_2", "tp"))
    placed = (
        P(SP, "tp"),
        P(SP, None),
        P(SP, None),
        P(SP, None, None),
        P(SP, None, "tp"),
        P(SP, None, "tp"),
        P(SP, "tp", None),
        P("tp", None),
        P(SP, "tp"),
        P("tp"),
        P(None, "tp"),
        P(SP, "tp"),
        P(SP, "tp"),
    )
    return jax.shard_map(
        per_device,
        mesh=finer,
        in_specs=placed,
        out_specs=(
            P(SP, None, "tp"),
            P(SP, None, "tp"),
            P(SP, "tp", None),
            P(TP_SP, None),
            P(SP, "tp"),
            P(SP, "tp"),
        ),
        check_vma=False,
    )
```
